128 devices in a mesh: sp: 32 (over z, y, core), tp: 4 (over x).
Axes of the slice: x: 4, y: 4, z: 4, core: 2. Of those that a mesh axis runs over, the one named last changes fastest.
Arguments:
- query_rows: bfloat16 [32768, 1024], P('sp', 'tp'), may hold values from -6 to 6
- key_rows: bfloat16 [32768, 1024], P('sp', 'tp'), may hold values from -6 to 6
- value_rows: bfloat16 [32768, 1024], P('sp', 'tp'), may hold values from -6 to 6
- input_gate: float32 [8, 32768], P('tp', 'sp'), may hold values from -4 to 255
- forget_gate: float32 [8, 32768], P('tp', 'sp'), may hold values from -3 to 20
- output_gate: bfloat16 [32768, 1024], P('sp', 'tp'), may hold values from -6 to 6
- documents: int32 [32768], P('sp'), may hold values from 0 to 7, never falling along the last dimension, each value on 1 to 6144 neighbouring positions
- residual: bfloat16 [32768, 2048], P(('sp', 'tp')), may hold values from -6 to 6
- out_weight: bfloat16 [1024, 2048], P('tp'), may hold values from -0.375 to 0.375
- norm_gain: bfloat16 [2048], replicated, may hold values from 0.099609375 to 1.8984375
- gate_weight: bfloat16 [2048, 5632], P('sp', 'tp'), may hold values from -0.125 to 0.125
- up_weight: bfloat16 [2048, 5632], P('sp', 'tp'), may hold values from -0.125 to 0.125
- down_weight: bfloat16 [5632, 2048], P('tp', 'sp'), may hold values from -0.15625 to 0.15625
Outputs:
- layer_out: bfloat16 [32768, 2048], P(('sp', 'tp'))
The draws below stay inside these ranges and needn't reach their ends.
Inputs may be any that keep to these rules, and one draw needn't show every extreme that they name: `documents`: document numbers never fall along the positions; each document covers 1 to 6144 positions and one covers exactly 6144.
All inputs are finite; a program needn't handle non-finite values.
Results may differ from the reference program's by a relative error of at most 0.013.
Values may be sent and summed in bfloat16 or wider, within the bound.
A program may use at most 128 MiB of HBM per device.

```python
import math
import jax
import jax.numpy as jnp
import numpy as np
from jax import lax

D = 2048
MEMORY_HEADS = 8
HD = 128
FF = 5632
BLOCK = 128
TOK_DEV = 1024
MW = 1024
PACKED_TOKENS = 32768
DOCS = 8
DOC_MOST = 6144
N_TP = 4


def draw_forget_gate(key, part):
    head_draw = jax.random.uniform(jax.random.fold_in(key, 11), (MEMORY_HEADS,), jnp.float32)
    slow_heads = head_draw < 0.5
    base_rate = jnp.where(slow_heads, 0.25 / PACKED_TOKENS, 1.0 / 40.0)
    block_count = PACKED_TOKENS // TOK_DEV
    block_scale = jnp.exp(jax.random.uniform(jax.random.fold_in(key, 12), (MEMORY_HEADS, block_count), jnp.float32, 0.0, math.log(3.0)))
    block_scale = jnp.repeat(block_scale, TOK_DEV, axis=1)
    jitter = 1.0 + 0.5 * jax.random.uniform(jax.random.fold_in(key, 13), (MEMORY_HEADS, PACKED_TOKENS), jnp.float32, -1.0, 1.0)
    spike_probability = base_rate[:, None] * block_scale * jitter
    spike_position = jax.random.randint(jax.random.fold_in(key, 14), (3,), 0, PACKED_TOKENS)
    spike_length = jax.random.uniform(jax.random.fold_in(key, 15), (MEMORY_HEADS, 3), jnp.float32, 0.22, 0.7)
    target_positions = jnp.arange(PACKED_TOKENS)
    match_count = (target_positions[None, :] == spike_position[:, None]).astype(jnp.float32)
    spike_probability = spike_probability + jnp.dot(spike_length, match_count)
    return -jnp.log(jnp.expm1(spike_probability))


def draw_input_gate(key, part):
    base = jnp.clip(jax.random.normal(jax.random.fold_in(key, 21), (MEMORY_HEADS, PACKED_TOKENS), jnp.float32), -4.0, 4.0)
    return base


def block_levels(rng, extent, pieces, smallest, largest):
    level, own = 1.0, jax.random.fold_in(rng, 6)
    for axis_at, blocks in pieces:
        steps = jnp.exp(jax.random.uniform(jax.random.fold_in(own, axis_at), (blocks,), jnp.float32, smallest / len(pieces), largest / len(pieces)))
        level = level * jnp.repeat(steps, extent[axis_at] // blocks).reshape([-1 if axis == axis_at else 1 for axis in range(len(extent))])
    return level


def length_profile(amount, total, bound, lean):
    loads = [(1 << 20) // math.isqrt(rank ** lean) + 1 for rank in range(2, amount + 1)]
    surplus, counts = total - bound - (amount - 1), [1] * (amount - 1)
    while surplus > 0:
        movable = [i for i in range(amount - 1) if counts[i] < bound]
        mass, remaining = sum([loads[i] for i in movable]), surplus
        for i in movable:
            more = min(bound - counts[i], max(1, remaining * loads[i] // mass), surplus)
            counts[i] = counts[i] + more
            surplus = surplus - more
    return np.array([bound] + counts)


def uneven(rng, count, total, reach, slope):
    if count == 2:
        one = jax.random.randint(rng, (), max(1, total - reach), min(reach, total - 1) + 1)
        return jnp.stack([one, total - one])
    sizes = jnp.asarray(length_profile(count, total, reach, slope), jnp.int32)
    twos = (count - 1) // 2
    source_of, sink = sizes[1:1 + 2 * twos:2], sizes[2:2 + 2 * twos:2]
    slack = jnp.minimum(source_of - 1, reach - sink)
    shifted = jax.random.randint(jax.random.fold_in(rng, 1), (twos,), 0, 1 << 20) % (slack + 1)
    sizes = sizes.at[1:1 + 2 * twos:2].set(source_of - shifted).at[2:2 + 2 * twos:2].set(sink + shifted)
    return sizes[jax.random.permutation(jax.random.fold_in(rng, 2), count)]


def centred(key, extent, deviation, limit, shards=(), dtype=jnp.bfloat16):
    level = block_levels(key, extent, shards, -0.22, 0.18) if shards else 1.0
    result = jax.random.normal(key, extent, jnp.float32) * deviation * level
    return jnp.minimum(jnp.maximum(result, -limit), limit).astype(dtype)


def setup_inputs(seed: int = 0) -> dict:
    splits = jax.random.split(jax.random.key(seed), 14)
    query_rows = centred(splits[0], (PACKED_TOKENS, MW), 1.0, 6.0, ((0, 32), (1, 4)))
    key_rows = centred(splits[1], (PACKED_TOKENS, MW), 1.0, 6.0, ((0, 32), (1, 4)))
    value_rows = centred(splits[2], (PACKED_TOKENS, MW), 1.0, 6.0, ((0, 32), (1, 4)))
    input_gate = draw_input_gate(jax.random.fold_in(splits[13], 71), 0)
    forget_gate = draw_forget_gate(jax.random.fold_in(splits[13], 71), 0)
    output_gate = centred(splits[5], (PACKED_TOKENS, MW), 1.5, 6.0, ((0, 32), (1, 4)))
    documents = jnp.searchsorted(jnp.cumsum(uneven(splits[6], DOCS, PACKED_TOKENS, DOC_MOST, 1)), jnp.arange(PACKED_TOKENS), side="right").astype(jnp.int32)
    residual = centred(splits[7], (PACKED_TOKENS, D), 1.0, 6.0, ((0, 128),))
    out_weight = centred(splits[8], (MW, D), (MW // 4) ** -0.5, 0.375, ((0, 4),))
    norm_gain = jnp.clip(1.0 + 0.18 * jax.random.normal(splits[9], (D,), jnp.float32), 0.099609375, 1.8984375).astype(jnp.bfloat16)
    gate_weight = centred(splits[10], (D, FF), D ** -0.5, 0.125, ((0, 32), (1, 4)))
    up_weight = centred(splits[11], (D, FF), D ** -0.5, 0.125, ((0, 32), (1, 4)))
    down_weight = centred(splits[12], (FF, D), (FF // 4) ** -0.5, 0.15625, ((0, 4), (1, 32)))
    return dict(query_rows=query_rows, key_rows=key_rows, value_rows=value_rows, input_gate=input_gate, forget_gate=forget_gate, output_gate=output_gate, documents=documents, residual=residual, out_weight=out_weight, norm_gain=norm_gain, gate_weight=gate_weight, up_weight=up_weight, down_weight=down_weight)


neg_large = -1e+30
norm_eps = 1e-06
highest = lax.Precision.HIGHEST

def block_step(carried, inputs):
    memory, normer, stab_prev, carry_doc = carried
    queries, key_float, value_float, gate_in, log_forget, docs = inputs
    cumlog = jnp.cumsum(log_forget, axis=1)
    length = docs.shape[0]
    target_positions = jnp.arange(length)
    same_doc = (docs[:, None] == docs[None, :]) & (target_positions[:, None] >= target_positions[None, :])
    log_weight = jnp.where(same_doc[None], cumlog[:, :, None] - cumlog[:, None, :] + gate_in[:, None, :], neg_large)
    carried_log = jnp.where((docs == carry_doc)[None, :], cumlog + stab_prev[:, None], neg_large)
    stabilizer = jnp.maximum(carried_log, lax.optimization_barrier(jnp.max(log_weight, axis=2)))
    scores = jnp.einsum('lhd,shd->hls', queries, key_float, precision=highest)
    weighted = scores * jnp.exp(log_weight - stabilizer[:, :, None])
    carried_scale = jnp.exp(carried_log - stabilizer)
    numerator = carried_scale[:, :, None] * jnp.einsum('lhd,hde->hle', queries, memory, precision=highest)
    numerator = numerator + jnp.einsum('hls,she->hle', weighted, value_float, precision=highest)
    denominator = carried_scale * jnp.einsum('lhd,hd->hl', queries, normer, precision=highest) + lax.optimization_barrier(jnp.sum(weighted, axis=2))
    outputs = numerator / jnp.maximum(jnp.abs(denominator), 1.0)[:, :, None]
    last_doc = docs[-1]
    inject_log = jnp.where((docs == last_doc)[None, :], cumlog[:, -1:] - cumlog + gate_in, neg_large)
    inject_max = lax.optimization_barrier(jnp.max(inject_log, axis=1))
    weights = jnp.exp(inject_log - inject_max[:, None])
    continues = carry_doc == last_doc
    stab_new = jnp.where(continues, jnp.maximum(cumlog[:, -1] + stab_prev, inject_max), inject_max)
    decay_scale = jnp.where(continues, jnp.exp(cumlog[:, -1] + stab_prev - stab_new), 0.0)
    inject = jnp.exp(inject_max - stab_new)
    memory_step = jnp.einsum('lhd,lhe->hde', key_float * weights.T[:, :, None], value_float, precision=highest)
    normer_step = jnp.einsum('hl,lhd->hd', weights, key_float, precision=highest)
    memory = decay_scale[:, None, None] * memory + inject[:, None, None] * memory_step
    normer = decay_scale[:, None] * normer + inject[:, None] * normer_step
    return ((memory, normer, stab_new, last_doc), jnp.transpose(outputs, (1, 0, 2)))

def run_blocks(queries, key_float, value_float, gate_in, log_forget, docs, start_state):
    length, heads, width = queries.shape
    count = length // BLOCK
    inputs = (queries.reshape(count, BLOCK, heads, width), key_float.reshape(count, BLOCK, heads, width), value_float.reshape(count, BLOCK, heads, width), jnp.moveaxis(gate_in.reshape(heads, count, BLOCK), 1, 0), jnp.moveaxis(log_forget.reshape(heads, count, BLOCK), 1, 0), docs.reshape(count, BLOCK))
    final, outputs = lax.scan(block_step, start_state, inputs)
    return (outputs.reshape(length, heads, width), final)

def reference(query_rows, key_rows, value_rows, input_gate, forget_gate, output_gate, documents, residual, out_weight, norm_gain, gate_weight, up_weight, down_weight):
    queries = query_rows.astype(jnp.float32).reshape(PACKED_TOKENS, MEMORY_HEADS, HD) * HD ** (-0.5)
    key_float = key_rows.astype(jnp.float32).reshape(PACKED_TOKENS, MEMORY_HEADS, HD)
    value_float = value_rows.astype(jnp.float32).reshape(PACKED_TOKENS, MEMORY_HEADS, HD)
    log_forget = jax.nn.log_sigmoid(forget_gate)
    start_state = (jnp.zeros((MEMORY_HEADS, HD, HD), jnp.float32), jnp.zeros((MEMORY_HEADS, HD), jnp.float32), jnp.full((MEMORY_HEADS,), neg_large, jnp.float32), jnp.array(-1, jnp.int32))
    cells, final = run_blocks(queries, key_float, value_float, input_gate, log_forget, documents, start_state)
    gated = (cells.reshape(PACKED_TOKENS, MW) * jax.nn.sigmoid(output_gate.astype(jnp.float32))).astype(jnp.bfloat16)
    projected = jnp.dot(gated, out_weight, preferred_element_type=jnp.float32)
    stream = residual.astype(jnp.float32) + projected
    normed = stream * lax.rsqrt(lax.optimization_barrier(jnp.mean(stream * stream, axis=1, keepdims=True)) + norm_eps)
    normed = (normed * norm_gain.astype(jnp.float32)).astype(jnp.bfloat16)
    gate_act = jnp.dot(normed, gate_weight, preferred_element_type=jnp.float32)
    up_act = jnp.dot(normed, up_weight, preferred_element_type=jnp.float32)
    hidden = (jax.nn.silu(gate_act) * up_act).astype(jnp.bfloat16)
    group = FF // N_TP
    down = jnp.zeros((PACKED_TOKENS, D), jnp.float32)
    for index in range(N_TP):
        partial_sum = jnp.dot(hidden[:, index * group:(index + 1) * group], down_weight[index * group:(index + 1) * group], preferred_element_type=jnp.float32)
        down = down + partial_sum.astype(jnp.bfloat16).astype(jnp.float32)
    return (stream + 0.5 * down).astype(jnp.bfloat16)
```

```python
import jax
import jax.numpy as jnp
from jax import lax
from jax.experimental import pallas as pl
from jax.experimental.pallas import tpu as pltpu
from jax.sharding import Mesh
from jax.sharding import PartitionSpec as P

HD = 128
SP = ("sp_0", "sp_1", "sp_2")
SP_TP = ("sp_0", "sp_1", "sp_2", "tp")
MESH = pl.DeviceIdType.MESH
BF = jnp.bfloat16
F32 = jnp.float32

NORM_EPS = 1e-06
NEG = -1e30
T = 1024
R = 256
D = 2048
FD = 1408
NJ = FD // 128
LOOK = 6
TILES = 3 * NJ
PARTS = ((0, 16, 8), (16, 17, 9))


def dot(a, b):
    return jnp.dot(a, b, preferred_element_type=F32)


def dot_nt(a, b):
    return lax.dot_general(a, b, (((1,), (1,)), ((), ())), preferred_element_type=F32)


def dot_tn(a, b):
    return lax.dot_general(a, b, (((0,), (0,)), ((), ())), preferred_element_type=F32)


def split(a):
    hi = a.astype(BF)
    return hi, (a - hi.astype(F32)).astype(BF)


def kernel(
    gates,
    gain,
    q_hbm,
    k_hbm,
    v_hbm,
    og_hbm,
    res_hbm,
    ow_hbm,
    wg_hbm,
    wu_hbm,
    wd_hbm,
    out,
    q,
    k,
    v,
    og,
    res,
    wg,
    wu,
    wd,
    w,
    ow,
    st_out,
    st_in,
    gate_out,
    gate_in,
    stream,
    rows,
    hid,
    part,
    mid,
    fin,
    vt,
    tt,
    arow,
    num,
    den,
    lsem,
    wss,
    wsr,
    oss,
    osr,
    sss,
    ssr,
    ass,
    asr,
    gss,
    gsr,
    rss,
    rsr,
):
    z, y, c, x = (lax.axis_index(n) for n in SP_TP)
    me = (z * 4 + y) * 2 + c

    def step(a, by):
        return lax.rem(a + by + 8, 4)

    def sp_device(ahead):
        i = lax.rem(me + ahead + 32, 32)
        return {"sp_0": i // 8, "sp_1": lax.rem(i // 2, 4), "sp_2": lax.rem(i, 2)}

    sibling = {"sp_2": 1 - c}
    peers = [sibling]
    for name, at in (("sp_0", z), ("sp_1", y), ("tp", x)):
        peers += [{name: step(at, 1)}, {name: step(at, -1)}]
    peers += [{"tp": step(x, 2)}]
    for d in range(1, LOOK + 1):
        peers += [sp_device(d), sp_device(-d)]

    local = []
    for n, (src, dst) in enumerate(
        (
            (k_hbm, k),
            (v_hbm, v),
            (wg_hbm, wg),
            (wu_hbm, wu),
            (wd_hbm, wd),
            (q_hbm, q),
            (ow_hbm, ow.at[x]),
            (og_hbm, og),
            (res_hbm, res),
        )
    ):
        copy = pltpu.make_async_copy(src, dst, lsem.at[n])
        copy.start()
        local.append(copy)
    in_k, in_v, in_wg, in_wu, in_wd, in_q, in_ow, in_og, in_res = local

    barrier = pltpu.get_barrier_semaphore()
    for peer in peers:
        pl.semaphore_signal(barrier, inc=1, device_id=peer, device_id_type=MESH)

    sent = []

    def remote(src, dst, send_sem, recv_sem, device):
        return pltpu.make_async_remote_copy(
            src_ref=src,
            dst_ref=dst,
            send_sem=send_sem,
            recv_sem=recv_sem,
            device_id=device,
            device_id_type=MESH,
        )

    def send(*args):
        copy = remote(*args)
        copy.start()
        sent.append(copy)

    def arrive(ref, send_sem, recv_sem):
        remote(ref, ref, send_sem, recv_sem, sibling).wait_recv()

    lane = lax.broadcasted_iota(jnp.int32, (8, 128), 1)
    row = lax.broadcasted_iota(jnp.int32, (8, 128), 0)
    docs = gates[32:40, :]
    last_lane = jnp.broadcast_to(docs[:, 127:128], (8, 128))
    heads = []
    vt[...] = jnp.zeros_like(vt)
    for h in range(2):
        cum = gates[16 + 8 * h : 24 + 8 * h, :]
        for s in (1, 2, 4, 8, 16, 32, 64):
            cum = cum + jnp.where(lane >= s, pltpu.roll(cum, s, 1), 0.0)
        upto = jnp.broadcast_to(cum[:, 127:128], (8, 128))
        for s in (1, 2, 4):
            upto = upto + jnp.where(row >= s, pltpu.roll(upto, s, 0), 0.0)
        cum = cum + jnp.where(row >= 1, pltpu.roll(upto, 1, 0), 0.0)
        a = gates[8 * h : 8 * h + 8, :] - cum
        m = a
        for s in (1, 2, 4, 8, 16, 32, 64):
            ok = (lane >= s) & (pltpu.roll(docs, s, 1) == docs)
            m = jnp.where(ok, jnp.maximum(m, pltpu.roll(m, s, 1)), m)
        e = jnp.broadcast_to(m[:, 127:128], (8, 128))
        for s in (1, 2, 4):
            ok = (row >= s) & (pltpu.roll(last_lane, s, 0) == last_lane)
            e = jnp.where(ok, jnp.maximum(e, pltpu.roll(e, s, 0)), e)
        ok = (row >= 1) & (pltpu.roll(last_lane, 1, 0) == docs)
        m = jnp.where(ok, jnp.maximum(m, pltpu.roll(e, 1, 0)), m)
        top = e[7:8, :]
        last = last_lane[7:8, :]
        weight = jnp.where(docs == last, jnp.exp(a - top), 0.0)
        arow[8 * h : 8 * h + 8, :] = a
        vt[8 * h : 8 * h + 8, :] = m
        vt[16 + 8 * h : 24 + 8 * h, :] = weight
        heads.append((top, upto[7:8, :], last))
    vt[32:40, :] = docs
    tt[...] = vt[...].T

    in_k.wait()
    in_v.wait()
    normers = []
    for h in range(2):
        cols = slice(h * HD, h * HD + HD)
        kw = jnp.concatenate(
            [
                k[128 * n : 128 * n + 128, cols].astype(F32)
                * tt[:, 16 + 8 * h + n : 17 + 8 * h + n]
                for n in range(8)
            ],
            axis=0,
        )
        hi, lo = split(kw)
        st_out[HD * h : HD * h + HD, :] = dot_tn(hi, v[:, cols]) + dot_tn(lo, v[:, cols])
        normers.append(jnp.sum(kw, axis=0, keepdims=True))
    st_out[256:264, :] = jnp.concatenate(
        normers
        + [heads[0][0], heads[1][0], heads[0][1], heads[1][1], heads[0][2], heads[0][2]],
        axis=0,
    )

    pl.semaphore_wait(barrier, len(peers))
    for d in range(1, LOOK + 1):
        send(st_out, st_in.at[d - 1], sss.at[d - 1], ssr.at[d - 1], sp_device(d))

    in_wg.wait()
    in_wu.wait()
    in_wd.wait()
    unit = (
        lax.broadcasted_iota(jnp.int32, (64, 64), 0) == lax.broadcasted_iota(jnp.int32, (64, 64), 1)
    ).astype(BF)
    for j in range(NJ):
        cols = slice(128 * j, 128 * j + 128)
        w[2 * j, z, y, c] = wg[:, cols]
        w[2 * j + 1, z, y, c] = wu[:, cols]
        w[2 * NJ + j, z, y, c] = dot_nt(unit, wd[cols, :]).astype(BF)

    def w_axes(p):
        return (("sp_0", z), ("sp_1", y)) if p == 0 else (("sp_1", y), ("sp_0", z))

    def w_at(p, first, count, uu, vv):
        zz, yy = (uu, vv) if p == 0 else (vv, uu)
        return w.at[pl.ds(first, count), zz, yy, c]

    def w_send(p, n, first, count, uu, vv, device):
        ref = w_at(p, first, count, uu, vv)
        send(ref, ref, wss.at[p, n], wsr.at[p, n], device)

    def w_arrive(p, n, first, count, uu, vv):
        arrive(w_at(p, first, count, uu, vv), wss.at[p, n], wsr.at[p, n])

    LINE = (0, -1, 1, 2)

    def w_spread(p, n):
        (_, uu), (vn, vv) = w_axes(p)
        first, count, _ = PARTS[p]
        for s, by in ((0, 1), (1, -1)):
            w_send(p, 4 + 4 * n + s, first, count, step(uu, LINE[n]), vv, {vn: step(vv, by)})

    def w_pass_on(p, n):
        (_, uu), (vn, vv) = w_axes(p)
        first, count, half = PARTS[p]
        k_at = step(uu, LINE[n])
        w_arrive(p, 4 + 4 * n, first, count, k_at, step(vv, -1))
        w_send(p, 6 + 4 * n, first, half, k_at, step(vv, -1), {vn: step(vv, 1)})
        w_arrive(p, 5 + 4 * n, first, count, k_at, step(vv, 1))
        w_send(p, 7 + 4 * n, first + half, count - half, k_at, step(vv, 1), {vn: step(vv, -1)})

    def w_line(p, n, get):
        (_, uu), _ = w_axes(p)
        first, count, _ = PARTS[p]
        k_at = step(uu, LINE[n])
        core = 1 - c if get else c
        span = pl.ds(first, count)
        ref = w.at[span, k_at, :, core] if p == 0 else w.at[span, :, k_at, core]
        if get:
            arrive(ref, wss.at[p, 20 + n], wsr.at[p, 20 + n])
        else:
            send(ref, ref, wss.at[p, 20 + n], wsr.at[p, 20 + n], sibling)

    def w_finish(p, n):
        (_, uu), (_, vv) = w_axes(p)
        first, count, half = PARTS[p]
        k_at = step(uu, LINE[n])
        w_arrive(p, 6 + 4 * n, first, half, k_at, step(vv, 2))
        w_arrive(p, 7 + 4 * n, first + half, count - half, k_at, step(vv, 2))
        w_line(p, n, False)

    def w_0(p):
        (un, uu), (_, vv) = w_axes(p)
        first, count, _ = PARTS[p]
        for s, by in ((0, 1), (1, -1)):
            w_send(p, s, first, count, uu, vv, {un: step(uu, by)})
        w_spread(p, 0)

    def w_1(p):
        (un, uu), (_, vv) = w_axes(p)
        first, count, half = PARTS[p]
        w_arrive(p, 0, first, count, step(uu, -1), vv)
        w_send(p, 2, first, half, step(uu, -1), vv, {un: step(uu, 1)})
        w_spread(p, 1)
        w_arrive(p, 1, first, count, step(uu, 1), vv)
        w_send(p, 3, first + half, count - half, step(uu, 1), vv, {un: step(uu, -1)})
        w_spread(p, 2)

    def w_2(p):
        (_, uu), (_, vv) = w_axes(p)
        first, count, half = PARTS[p]
        w_arrive(p, 2, first, half, step(uu, 2), vv)
        w_arrive(p, 3, first + half, count - half, step(uu, 2), vv)
        w_spread(p, 3)

    right, left, across = {"tp": step(x, 1)}, {"tp": step(x, -1)}, {"tp": step(x, 2)}
    x_r, x_l, x_a = step(x, 1), step(x, -1), step(x, 2)

    def o_at(slot, part_first, count):
        return ow.at[slot, pl.ds(c * 128 + part_first, count)]

    def o_send(n, slot, first, count, device):
        send(o_at(slot, first, count), o_at(slot, first, count), oss.at[n], osr.at[n], device)

    def o_arrive(n, slot, first, count):
        arrive(o_at(slot, first, count), oss.at[n], osr.at[n])

    in_ow.wait()
    o_send(0, x, 0, 128, right)
    o_send(1, x, 0, 128, left)
    w_0(0)
    w_0(1)

    in_q.wait()
    scale = HD**-0.5
    for h in range(2):
        cols = slice(h * HD, h * HD + HD)
        for i in range(4):
            at = slice(256 * i, 256 * i + 256)
            m_col, d_col = (
                jnp.concatenate([tt[:, n + 2 * i : n + 2 * i + 1], tt[:, n + 2 * i + 1 : n + 2 * i + 2]], axis=0)
                for n in (8 * h, 32)
            )
            total = jnp.zeros((256, 1), F32)
            acc = jnp.zeros((256, HD), F32)
            for j in range(i + 1):
                keys = slice(256 * j, 256 * j + 256)
                a_row = jnp.concatenate(
                    [arow[8 * h + 2 * j + s : 8 * h + 2 * j + s + 1, :] for s in range(2)], axis=1
                )
                d_row = jnp.concatenate(
                    [gates[32 + 2 * j + s : 33 + 2 * j + s, :] for s in range(2)], axis=1
                )
                ok = d_col == d_row
                if i == j:
                    ok = ok & (
                        lax.broadcasted_iota(jnp.int32, (256, 256), 0)
                        >= lax.broadcasted_iota(jnp.int32, (256, 256), 1)
                    )
                p = jnp.where(ok, dot_nt(q[at, cols], k[keys, cols]) * jnp.exp(a_row - m_col), 0.0)
                total = total + jnp.sum(p, axis=1, keepdims=True)
                hi, lo = split(p)
                acc = acc + (dot(hi, v[keys, cols]) + dot(lo, v[keys, cols]))
            num[at, cols] = acc
            den[at, cols] = jnp.broadcast_to(total, (256, HD))

    for d in range(1, LOOK + 1):
        arrive(st_in.at[d - 1], sss.at[d - 1], ssr.at[d - 1])
    in_og.wait()
    one_back = st_in[0, 262:263, :]
    carry_doc = jnp.where(me > 0, one_back, -1.0)[:, :1]
    for h in range(2):
        cols = slice(h * HD, h * HD + HD)
        passed = jnp.zeros((1, 128), F32)
        levels = []
        stab = jnp.full((1, 128), NEG, F32)
        for d in range(1, LOOK + 1):
            passed = passed + st_in[d - 1, 260 + h : 261 + h, :]
            ok = (st_in[d - 1, 262:263, :] == one_back) & (me >= d)
            level = jnp.where(ok, st_in[d - 1, 258 + h : 259 + h, :] + passed, NEG)
            levels.append(level)
            stab = jnp.maximum(stab, level)
        memory = jnp.zeros((HD, HD), F32)
        normer = jnp.zeros((1, HD), F32)
        for d in range(1, LOOK + 1):
            share = jnp.where(levels[d - 1] > 0.5 * NEG, jnp.exp(levels[d - 1] - stab), 0.0)
            memory = memory + share * st_in[d - 1, HD * h : HD * h + HD, :]
            normer = normer + share * st_in[d - 1, 256 + h : 257 + h, :]
        mem_hi, mem_lo = split(memory)
        before = stab[:, :1]
        for i in range(4):
            at = slice(256 * i, 256 * i + 256)
            m_col, d_col = (
                jnp.concatenate([tt[:, n + 2 * i : n + 2 * i + 1], tt[:, n + 2 * i + 1 : n + 2 * i + 2]], axis=0)
                for n in (8 * h, 32)
            )
            goes_on = d_col == carry_doc
            both = jnp.where(goes_on, jnp.maximum(m_col, before), m_col)
            scale_in = jnp.exp(m_col - both)
            scale_by = jnp.where(goes_on, jnp.exp(before - both), 0.0)
            queries = q[at, cols]
            from_norm = jnp.sum(queries.astype(F32) * normer, axis=1, keepdims=True)
            above = scale_in * num[at, cols] + scale_by * (dot(queries, mem_hi) + dot(queries, mem_lo))
            below = scale_in * den[at, cols] + scale_by * from_norm
            cell = above * scale / jnp.maximum(jnp.abs(below) * scale, 1.0)
            gate = 1.0 / (1.0 + jnp.exp(-og[at, cols].astype(F32)))
            gate_out[i, :, cols] = (cell * gate).astype(BF)

    for n, (device, slot) in enumerate(((right, x_r), (left, x_l), (across, x_a))):
        send(gate_out.at[slot], gate_in.at[x], ass.at[n], asr.at[n], device)
    gate_in[x] = gate_out[x]

    w_1(0)
    w_1(1)
    o_arrive(0, x_l, 0, 128)
    o_send(2, x_l, 0, 64, right)
    o_arrive(1, x_r, 0, 128)
    o_send(3, x_r, 64, 64, left)
    for n, slot in ((4, x_l), (5, x_r)):
        o_send(n, slot, 0, 128, sibling)
    w_2(0)
    w_2(1)
    w_pass_on(0, 0)
    w_pass_on(1, 0)
    o_arrive(2, x_a, 0, 64)
    o_arrive(3, x_a, 64, 64)
    o_send(6, x_a, 0, 128, sibling)
    for n, slot in enumerate((x_l, x_r, x_a)):
        arrive(gate_in.at[slot], ass.at[n], asr.at[n])
        arrive(ow.at[slot, pl.ds((1 - c) * 128, 128)], oss.at[4 + n], osr.at[4 + n])

    in_res.wait()

    def project(n, squares):
        cols = pl.ds(pl.multiple_of(n * 256, 256), 256)
        acc = res[:, cols].astype(F32)
        acc = acc + (
            (dot(gate_in[0], ow[0, :, cols]) + dot(gate_in[1], ow[1, :, cols]))
            + (dot(gate_in[2], ow[2, :, cols]) + dot(gate_in[3], ow[3, :, cols]))
        )
        stream[:, cols] = acc
        return squares + (acc[:, :128] * acc[:, :128] + acc[:, 128:] * acc[:, 128:])

    squares = lax.fori_loop(0, D // 256, project, jnp.zeros((R, 128), F32))
    inverse = lax.rsqrt(jnp.sum(squares, axis=1, keepdims=True) / D + NORM_EPS)

    def normalize(n, carry):
        cols = pl.ds(pl.multiple_of(n * 256, 256), 256)
        rows[x, :, cols] = (stream[:, cols] * inverse * gain[:, cols].astype(F32)).astype(BF)
        return carry

    lax.fori_loop(0, D // 256, normalize, 0)

    def r_at(slot, half):
        return rows.at[slot, pl.ds(128 * half, 128)]

    def r_send(n, slot, half, device):
        send(r_at(slot, half), r_at(slot, half), gss.at[n], gsr.at[n], device)

    def r_arrive(n, slot, half):
        arrive(r_at(slot, half), gss.at[n], gsr.at[n])

    r_send(0, x, 0, right)
    r_send(1, x, 1, left)
    r_send(2, x, 1, right)
    r_send(3, x, 0, left)

    for n in (1, 2):
        w_pass_on(0, n)
        w_pass_on(1, n)
    r_arrive(0, x_l, 0)
    r_send(4, x_l, 0, right)
    r_arrive(1, x_r, 1)
    r_send(5, x_r, 1, left)
    w_pass_on(0, 3)
    w_pass_on(1, 3)
    for n in range(4):
        w_finish(0, n)
        w_finish(1, n)
    for n in range(4):
        w_line(0, n, True)
        w_line(1, n, True)

    def widen(slot):
        def one(j, carry):
            both = jnp.concatenate(
                [w[2 * j].reshape(D, 128), w[2 * j + 1].reshape(D, 128)], axis=1
            )
            acts = dot(rows[slot], both)
            gate_act, up_act = acts[:, :128], acts[:, 128:]
            cols = pl.ds(pl.multiple_of(j * 128, 128), 128)
            hid[slot, :, cols] = (gate_act * (1.0 / (1.0 + jnp.exp(-gate_act))) * up_act).astype(BF)
            return carry

        lax.fori_loop(0, NJ, one, 0)

    def narrow(slot, store):
        def one(n, carry):
            down = jnp.concatenate(
                [
                    w[2 * NJ + j, n // 2, pl.ds(2 * lax.rem(n, 2), 2)].reshape(256, 128)
                    for j in range(NJ)
                ],
                axis=1,
            )
            store(pl.ds(pl.multiple_of(n * 256, 256), 256), dot_nt(hid[slot], down))
            return carry

        lax.fori_loop(0, D // 256, one, 0)

    def keep(n):
        def store(cols, value):
            part[n, :, cols] = value.astype(BF)

        return store

    widen(x)
    r_arrive(2, x_l, 1)
    widen(x_l)
    r_arrive(3, x_r, 0)
    widen(x_r)
    r_arrive(4, x_a, 0)
    r_arrive(5, x_a, 1)
    widen(x_a)

    up_half, low_half = pl.ds(0, 128), pl.ds(128, 128)
    narrow(x_a, keep(0))
    send(part.at[0, up_half], mid.at[0], rss.at[0], rsr.at[0], right)
    send(part.at[0, low_half], mid.at[1], rss.at[1], rsr.at[1], left)
    narrow(x_r, keep(1))
    send(part.at[1, low_half], fin.at[0, low_half], rss.at[2], rsr.at[2], right)
    narrow(x_l, keep(2))
    send(part.at[2, up_half], fin.at[1, up_half], rss.at[3], rsr.at[3], left)
    arrive(mid.at[0], rss.at[0], rsr.at[0])
    part[1, up_half] = (part[1, up_half].astype(F32) + mid[0].astype(F32)).astype(BF)
    send(part.at[1, up_half], fin.at[0, up_half], rss.at[4], rsr.at[4], right)
    arrive(mid.at[1], rss.at[1], rsr.at[1])
    part[2, low_half] = (part[2, low_half].astype(F32) + mid[1].astype(F32)).astype(BF)
    send(part.at[2, low_half], fin.at[1, low_half], rss.at[5], rsr.at[5], left)

    def own(cols, value):
        stream[:, cols] = stream[:, cols] + 0.5 * value

    narrow(x, own)
    arrive(fin.at[0, low_half], rss.at[2], rsr.at[2])
    arrive(fin.at[1, up_half], rss.at[3], rsr.at[3])
    arrive(fin.at[0, up_half], rss.at[4], rsr.at[4])
    arrive(fin.at[1, low_half], rss.at[5], rsr.at[5])

    def finish(n, carry):
        cols = pl.ds(pl.multiple_of(n * 256, 256), 256)
        others = fin[0, :, cols].astype(F32) + fin[1, :, cols].astype(F32)
        out[:, cols] = (stream[:, cols] + 0.5 * others).astype(BF)
        return carry

    lax.fori_loop(0, D // 256, finish, 0)
    for copy in sent:
        copy.wait_send()


def body(
    query_rows,
    key_rows,
    value_rows,
    input_gate,
    forget_gate,
    output_gate,
    documents,
    residual,
    out_weight,
    norm_gain,
    gate_weight,
    up_weight,
    down_weight,
):
    gates = jnp.concatenate(
        [
            input_gate.reshape(16, 128),
            jax.nn.log_sigmoid(forget_gate).reshape(16, 128),
            documents.astype(F32).reshape(8, 128),
        ],
        axis=0,
    )
    vmem = pl.BlockSpec(memory_space=pltpu.VMEM)
    hbm = pl.BlockSpec(memory_space=pl.ANY)
    dma = pltpu.SemaphoreType.DMA
    return pl.pallas_call(
        kernel,
        out_shape=jax.ShapeDtypeStruct((R, D), BF),
        in_specs=[vmem] * 2 + [hbm] * 9,
        out_specs=vmem,
        scratch_shapes=[
            pltpu.VMEM((T, 256), BF),
            pltpu.VMEM((T, 256), BF),
            pltpu.VMEM((T, 256), BF),
            pltpu.VMEM((T, 256), BF),
            pltpu.VMEM((R, D), BF),
            pltpu.VMEM((64, FD), BF),
            pltpu.VMEM((64, FD), BF),
            pltpu.VMEM((FD, 64), BF),
            pltpu.VMEM((TILES, 4, 4, 2, 64, 128), BF),
            pltpu.VMEM((4, 256, D), BF),
            pltpu.VMEM((264, 128), F32),
            pltpu.VMEM((LOOK, 264, 128), F32),
            pltpu.VMEM((4, R, 256), BF),
            pltpu.VMEM((4, R, 256), BF),
            pltpu.VMEM((R, D), F32),
            pltpu.VMEM((4, R, D), BF),
            pltpu.VMEM((4, R, FD), BF),
            pltpu.VMEM((3, R, D), BF),
            pltpu.VMEM((2, 128, D), BF),
            pltpu.VMEM((2, R, D), BF),
            pltpu.VMEM((128, 128), F32),
            pltpu.VMEM((128, 128), F32),
            pltpu.VMEM((16, 128), F32),
            pltpu.VMEM((T, 256), F32),
            pltpu.VMEM((T, 256), F32),
            dma((9,)),
            dma((2, 24)),
            dma((2, 24)),
            dma((7,)),
            dma((7,)),
            dma((LOOK,)),
            dma((LOOK,)),
            dma((3,)),
            dma((3,)),
            dma((6,)),
            dma((6,)),
            dma((6,)),
            dma((6,)),
        ],
        compiler_params=pltpu.CompilerParams(
            collective_id=0, has_side_effects=True, vmem_limit_bytes=62 * 1024 * 1024
        ),
    )(
        gates,
        norm_gain.reshape(1, D),
        query_rows,
        key_rows,
        value_rows,
        output_gate,
        residual,
        out_weight,
        gate_weight,
        up_weight,
        down_weight,
    )


def solution(mesh):
    torus = Mesh(mesh.devices.reshape(4, 4, 2, mesh.shape["tp"]), SP_TP)
    in_specs = (
        P(SP, "tp"),
        P(SP, "tp"),
        P(SP, "tp"),
        P("tp", SP),
        P("tp", SP),
        P(SP, "tp"),
        P(SP),
        P(SP_TP, None),
        P("tp", None),
        P(),
        P(SP, "tp"),
        P(SP, "tp"),
        P("tp", SP),
    )
    out_specs = P(SP_TP, None)
    return jax.shard_map(body, mesh=torus, in_specs=in_specs, out_specs=out_specs, check_vma=False)
```

```python
import jax
import jax.numpy as jnp
from jax import lax
from jax.experimental import pallas as pl
from jax.experimental.pallas import tpu as pltpu
from jax.sharding import Mesh
from jax.sharding import PartitionSpec as P

HD = 128
SP = ("sp_0", "sp_1", "sp_2")
SP_TP = ("sp_0", "sp_1", "sp_2", "tp")
MESH = pl.DeviceIdType.MESH
BF = jnp.bfloat16
F32 = jnp.float32

NORM_EPS = 1e-06
NEG = -1e30
T = 1024
R = 256
D = 2048
FD = 1408
NJ = FD // 128
LOOK = 3
TILES = 3 * NJ
PARTS = ((0, 16, 8), (16, 17, 9))


def dot(a, b):
    return jnp.dot(a, b, preferred_element_type=F32)


def dot_nt(a, b):
    return lax.dot_general(a, b, (((1,), (1,)), ((), ())), preferred_element_type=F32)


def dot_tn(a, b):
    return lax.dot_general(a, b, (((0,), (0,)), ((), ())), preferred_element_type=F32)


def split(a):
    hi = a.astype(BF)
    return hi, (a - hi.astype(F32)).astype(BF)


def kernel(
    in_gate,
    forget,
    doc_ref,
    gain,
    q_hbm,
    k_hbm,
    v_hbm,
    og_hbm,
    res_hbm,
    ow_hbm,
    wg_hbm,
    wu_hbm,
    wd_hbm,
    out,
    q,
    k,
    v,
    og,
    res,
    wg,
    wu,
    wd,
    w,
    ow,
    st_out,
    st_twin,
    mem_out,
    meta_out,
    mem_in,
    meta_in,
    gate_out,
    gate_in,
    stream,
    rows,
    hid,
    part,
    mid,
    fin,
    vt,
    tt,
    arow,
    drow,
    gsc,
    vones,
    numden,
    opened,
    lsem,
    wss,
    wsr,
    oss,
    osr,
    sss,
    ssr,
    ass,
    asr,
    gss,
    gsr,
    rss,
    rsr,
):
    z, y, c, x = (lax.axis_index(n) for n in SP_TP)

    def step(a, by):
        return lax.rem(a + by + 8, 4)

    chip = z * 4 + y

    def chip_ahead(by):
        i = lax.rem(chip + by + 16, 16)
        return {"sp_0": i // 4, "sp_1": lax.rem(i, 4)}

    sibling = {"sp_2": 1 - c}
    peers = [sibling]
    for name, at in (("sp_0", z), ("sp_1", y), ("tp", x)):
        peers += [{name: step(at, 1)}, {name: step(at, -1)}]
    peers += [{"tp": step(x, 2)}]
    for d in range(1, LOOK + 1):
        peers += [chip_ahead(d), chip_ahead(-d)]

    local = []
    for n, (src, dst) in enumerate(
        (
            (k_hbm, k),
            (v_hbm, v),
            (wg_hbm, wg),
            (wu_hbm, wu),
            (wd_hbm, wd),
            (q_hbm, q),
            (ow_hbm, ow.at[x]),
            (og_hbm, og),
            (res_hbm, res),
        )
    ):
        copy = pltpu.make_async_copy(src, dst, lsem.at[n])
        copy.start()
        local.append(copy)
    in_k, in_v, in_wg, in_wu, in_wd, in_q, in_ow, in_og, in_res = local

    barrier = pltpu.get_barrier_semaphore()
    for peer in peers:
        pl.semaphore_signal(barrier, inc=1, device_id=peer, device_id_type=MESH)

    sent = []

    def remote(src, dst, send_sem, recv_sem, device):
        return pltpu.make_async_remote_copy(
            src_ref=src,
            dst_ref=dst,
            send_sem=send_sem,
            recv_sem=recv_sem,
            device_id=device,
            device_id_type=MESH,
        )

    def send(*args):
        copy = remote(*args)
        copy.start()
        sent.append(copy)

    def arrive(ref, send_sem, recv_sem):
        remote(ref, ref, send_sem, recv_sem, sibling).wait_recv()

    lane = lax.broadcasted_iota(jnp.int32, (8, 128), 1)
    row = lax.broadcasted_iota(jnp.int32, (8, 128), 0)
    docs = doc_ref[...].astype(F32)
    drow[...] = docs
    gsc[...] = gain[...].astype(F32)
    last_lane = jnp.broadcast_to(docs[:, 127:128], (8, 128))
    heads = []
    vt[...] = jnp.zeros_like(vt)

    def eight_rows(ref, h):
        return jnp.concatenate([ref[h : h + 1, 128 * n : 128 * n + 128] for n in range(8)], axis=0)

    for h in range(2):
        cum = eight_rows(forget, h)
        cum = jnp.minimum(cum, 0.0) - jnp.log1p(jnp.exp(-jnp.abs(cum)))
        for s in (1, 2, 4, 8, 16, 32, 64):
            cum = cum + jnp.where(lane >= s, pltpu.roll(cum, s, 1), 0.0)
        upto = jnp.broadcast_to(cum[:, 127:128], (8, 128))
        for s in (1, 2, 4):
            upto = upto + jnp.where(row >= s, pltpu.roll(upto, s, 0), 0.0)
        cum = cum + jnp.where(row >= 1, pltpu.roll(upto, 1, 0), 0.0)
        a = eight_rows(in_gate, h) - cum
        m = a
        for s in (1, 2, 4, 8, 16, 32, 64):
            ok = (lane >= s) & (pltpu.roll(docs, s, 1) == docs)
            m = jnp.where(ok, jnp.maximum(m, pltpu.roll(m, s, 1)), m)
        e = jnp.broadcast_to(m[:, 127:128], (8, 128))
        for s in (1, 2, 4):
            ok = (row >= s) & (pltpu.roll(last_lane, s, 0) == last_lane)
            e = jnp.where(ok, jnp.maximum(e, pltpu.roll(e, s, 0)), e)
        ok = (row >= 1) & (pltpu.roll(last_lane, 1, 0) == docs)
        m = jnp.where(ok, jnp.maximum(m, pltpu.roll(e, 1, 0)), m)
        top = e[7:8, :]
        last = last_lane[7:8, :]
        weight = jnp.where(docs == last, jnp.exp(a - top), 0.0)
        arow[8 * h : 8 * h + 8, :] = a
        vt[8 * h : 8 * h + 8, :] = m
        vt[16 + 8 * h : 24 + 8 * h, :] = weight
        total = upto[7:8, :]
        heads.append((top + total, total, m))
    vt[32:40, :] = docs
    tt[...] = vt[...].T

    in_k.wait()
    in_v.wait()
    normers = []
    for h in range(2):
        cols = slice(h * HD, h * HD + HD)
        kw = jnp.concatenate(
            [
                k[128 * n : 128 * n + 128, cols].astype(F32)
                * tt[:, 16 + 8 * h + n : 17 + 8 * h + n]
                for n in range(8)
            ],
            axis=0,
        )
        hi, lo = split(kw)
        st_out[HD * h : HD * h + HD, :] = dot_tn(hi, v[:, cols]) + dot_tn(lo, v[:, cols])
        normers.append(jnp.sum(kw, axis=0, keepdims=True))
    st_out[256:264, :] = jnp.concatenate(
        normers
        + [heads[0][0], heads[1][0], heads[0][1], heads[1][1], last, last],
        axis=0,
    )

    pl.semaphore_wait(barrier, len(peers))
    send(st_out, st_twin, sss.at[0], ssr.at[0], sibling)

    in_wg.wait()
    in_wu.wait()
    in_wd.wait()
    for j in range(NJ):
        cols = slice(128 * j, 128 * j + 128)
        w[2 * j, z, y, c] = wg[:, cols]
        w[2 * j + 1, z, y, c] = wu[:, cols]
        w[2 * NJ + j, z, y, c] = wd[:, cols]

    arrive(st_twin, sss.at[0], ssr.at[0])
    first_core = c == 0
    mine, twin = st_out[256:264, :], st_twin[256:264, :]
    early = jnp.where(first_core, mine, twin)
    late = jnp.where(first_core, twin, mine)
    goes = early[6:7, :] == late[6:7, :]
    meta = [None] * 8
    for h in range(2):
        span = slice(HD * h, HD * h + HD)
        one = jnp.where(goes, early[2 + h : 3 + h, :] + late[4 + h : 5 + h, :], NEG)
        two = late[2 + h : 3 + h, :]
        stab = jnp.maximum(one, two)
        share_one = jnp.where(goes, jnp.exp(one - stab), 0.0)
        share_two = jnp.exp(two - stab)
        share_mine = jnp.where(first_core, share_one, share_two)
        share_twin = jnp.where(first_core, share_two, share_one)
        mem_out[span, :] = (share_mine * st_out[span, :] + share_twin * st_twin[span, :]).astype(BF)
        meta[h] = share_mine * mine[h : h + 1, :] + share_twin * twin[h : h + 1, :]
        meta[2 + h] = stab
        meta[4 + h] = early[4 + h : 5 + h, :] + late[4 + h : 5 + h, :]
    meta[6] = meta[7] = late[6:7, :]
    meta_out[...] = jnp.concatenate(meta, axis=0)
    for d in range(1, LOOK + 1):
        send(meta_out, meta_in.at[d - 1], sss.at[2 * d], ssr.at[2 * d], chip_ahead(d))
        send(mem_out, mem_in.at[d - 1], sss.at[2 * d - 1], ssr.at[2 * d - 1], chip_ahead(d))

    def w_axes(p):
        return (("sp_0", z), ("sp_1", y)) if p == 0 else (("sp_1", y), ("sp_0", z))

    def w_at(p, first, count, uu, vv):
        zz, yy = (uu, vv) if p == 0 else (vv, uu)
        return w.at[pl.ds(first, count), zz, yy, c]

    def w_send(p, n, first, count, uu, vv, device):
        ref = w_at(p, first, count, uu, vv)
        send(ref, ref, wss.at[p, n], wsr.at[p, n], device)

    def w_arrive(p, n, first, count, uu, vv):
        arrive(w_at(p, first, count, uu, vv), wss.at[p, n], wsr.at[p, n])

    LINE = (0, -1, 1, 2)

    def w_spread(p, n):
        (_, uu), (vn, vv) = w_axes(p)
        first, count, _ = PARTS[p]
        for s, by in ((0, 1), (1, -1)):
            w_send(p, 4 + 4 * n + s, first, count, step(uu, LINE[n]), vv, {vn: step(vv, by)})

    def w_pass_on(p, n):
        (_, uu), (vn, vv) = w_axes(p)
        first, count, half = PARTS[p]
        k_at = step(uu, LINE[n])
        w_arrive(p, 4 + 4 * n, first, count, k_at, step(vv, -1))
        w_send(p, 6 + 4 * n, first, half, k_at, step(vv, -1), {vn: step(vv, 1)})
        w_arrive(p, 5 + 4 * n, first, count, k_at, step(vv, 1))
        w_send(p, 7 + 4 * n, first + half, count - half, k_at, step(vv, 1), {vn: step(vv, -1)})

    def w_line(p, n, get):
        (_, uu), _ = w_axes(p)
        first, count, _ = PARTS[p]
        k_at = step(uu, LINE[n])
        core = 1 - c if get else c
        span = pl.ds(first, count)
        ref = w.at[span, k_at, :, core] if p == 0 else w.at[span, :, k_at, core]
        if get:
            arrive(ref, wss.at[p, 20 + n], wsr.at[p, 20 + n])
        else:
            send(ref, ref, wss.at[p, 20 + n], wsr.at[p, 20 + n], sibling)

    def w_finish(p, n):
        (_, uu), (_, vv) = w_axes(p)
        first, count, half = PARTS[p]
        k_at = step(uu, LINE[n])
        w_arrive(p, 6 + 4 * n, first, half, k_at, step(vv, 2))
        w_arrive(p, 7 + 4 * n, first + half, count - half, k_at, step(vv, 2))
        w_line(p, n, False)

    def w_0(p):
        (un, uu), (_, vv) = w_axes(p)
        first, count, _ = PARTS[p]
        for s, by in ((0, 1), (1, -1)):
            w_send(p, s, first, count, uu, vv, {un: step(uu, by)})
        w_spread(p, 0)

    def w_1(p):
        (un, uu), (_, vv) = w_axes(p)
        first, count, half = PARTS[p]
        w_arrive(p, 0, first, count, step(uu, -1), vv)
        w_send(p, 2, first, half, step(uu, -1), vv, {un: step(uu, 1)})
        w_spread(p, 1)
        w_arrive(p, 1, first, count, step(uu, 1), vv)
        w_send(p, 3, first + half, count - half, step(uu, 1), vv, {un: step(uu, -1)})
        w_spread(p, 2)

    def w_2(p):
        (_, uu), (_, vv) = w_axes(p)
        first, count, half = PARTS[p]
        w_arrive(p, 2, first, half, step(uu, 2), vv)
        w_arrive(p, 3, first + half, count - half, step(uu, 2), vv)
        w_spread(p, 3)

    right, left, across = {"tp": step(x, 1)}, {"tp": step(x, -1)}, {"tp": step(x, 2)}
    x_r, x_l, x_a = step(x, 1), step(x, -1), step(x, 2)

    def o_at(slot, part_first, count):
        return ow.at[slot, pl.ds(c * 128 + part_first, count)]

    def o_send(n, slot, first, count, device):
        send(o_at(slot, first, count), o_at(slot, first, count), oss.at[n], osr.at[n], device)

    def o_arrive(n, slot, first, count):
        arrive(o_at(slot, first, count), oss.at[n], osr.at[n])

    in_ow.wait()
    o_send(0, x, 0, 128, right)
    o_send(1, x, 0, 128, left)
    w_0(0)
    w_0(1)

    in_q.wait()
    for h in range(2):
        vones[h, :, :HD] = v[:, HD * h : HD * h + HD]
        vones[h, :, HD:] = jnp.ones((T, HD), BF)

    def column(n):
        return jnp.concatenate([tt[:, n : n + 1], tt[:, n + 1 : n + 2]], axis=0)

    for h in range(2):
        cols = slice(h * HD, h * HD + HD)
        for i in range(4):
            at = slice(256 * i, 256 * i + 256)
            m_col, d_col = column(8 * h + 2 * i), column(32 + 2 * i)
            acc = jnp.zeros((256, 2 * HD), F32)
            for j in range(i + 1):
                keys = slice(256 * j, 256 * j + 256)
                a_row, d_row = (
                    jnp.concatenate([ref[n + 2 * j : n + 2 * j + 1, :], ref[n + 2 * j + 1 : n + 2 * j + 2, :]], axis=1)
                    for ref, n in ((arow, 8 * h), (drow, 0))
                )
                ok = d_col == d_row
                if i == j:
                    ok = ok & (
                        lax.broadcasted_iota(jnp.int32, (256, 256), 0)
                        >= lax.broadcasted_iota(jnp.int32, (256, 256), 1)
                    )
                p = jnp.where(ok, dot_nt(q[at, cols], k[keys, cols]) * jnp.exp(a_row - m_col), 0.0)
                hi, lo = split(p)
                acc = acc + (dot(hi, vones[h, keys, :]) + dot(lo, vones[h, keys, :]))
            numden[h, at, :] = acc
    in_og.wait()
    for i in range(4):
        at = slice(256 * i, 256 * i + 256)
        opened[at, :] = 1.0 / (1.0 + jnp.exp(-og[at, :].astype(F32)))

    for d in range(1, LOOK + 1):
        arrive(meta_in.at[d - 1], sss.at[2 * d], ssr.at[2 * d])
        arrive(mem_in.at[d - 1], sss.at[2 * d - 1], ssr.at[2 * d - 1])
    second_core = c == 1
    one_back = meta_in[0, 6:7, :]
    carry_doc = jnp.where(second_core, twin[6:7, :], jnp.where(chip > 0, one_back, -1.0))
    scale = HD**-0.5
    memories = []
    for h in range(2):
        passed = jnp.where(second_core, twin[4 + h : 5 + h, :], 0.0)
        levels = [jnp.where(second_core, twin[2 + h : 3 + h, :], NEG)]
        for d in range(1, LOOK + 1):
            ok = (meta_in[d - 1, 6:7, :] == carry_doc) & (chip >= d)
            levels.append(jnp.where(ok, meta_in[d - 1, 2 + h : 3 + h, :] + passed, NEG))
            passed = passed + meta_in[d - 1, 4 + h : 5 + h, :]
        stab = levels[0]
        for level in levels[1:]:
            stab = jnp.maximum(stab, level)
        shares = [jnp.where(level > 0.5 * NEG, jnp.exp(level - stab), 0.0) for level in levels]
        memory = shares[0] * st_twin[HD * h : HD * h + HD, :]
        normer = shares[0] * twin[h : h + 1, :]
        for d in range(1, LOOK + 1):
            memory = memory + shares[d] * mem_in[d - 1, HD * h : HD * h + HD, :].astype(F32)
            normer = normer + shares[d] * meta_in[d - 1, h : h + 1, :]
        memories.append(memory)
        m = heads[h][2]
        goes_on = docs == carry_doc
        both = jnp.where(goes_on, jnp.maximum(m, stab), m)
        vt[8 * h : 8 * h + 8, :] = jnp.exp(m - both) * scale
        vt[16 + 8 * h : 24 + 8 * h, :] = jnp.where(goes_on, jnp.exp(stab - both), 0.0) * scale
        vt[32 + 8 * h : 40 + 8 * h, :] = jnp.broadcast_to(normer, (8, HD))
    tt[...] = vt[...].T
    for h in range(2):
        cols = slice(h * HD, h * HD + HD)
        normer = jnp.broadcast_to(tt[:, 32 + 8 * h : 33 + 8 * h], (HD, HD))
        parts = [jnp.concatenate(pair, axis=1) for pair in zip(split(memories[h]), split(normer))]
        for i in range(4):
            at = slice(256 * i, 256 * i + 256)
            scale_in, scale_by = column(8 * h + 2 * i), column(16 + 8 * h + 2 * i)
            queries = q[at, cols]
            both = scale_in * numden[h, at, :] + scale_by * (dot(queries, parts[0]) + dot(queries, parts[1]))
            cell = both[:, :HD] / jnp.maximum(jnp.abs(both[:, HD:]), 1.0)
            gate_out[i, :, cols] = (cell * opened[at, cols]).astype(BF)

    for n, (device, slot) in enumerate(((right, x_r), (left, x_l), (across, x_a))):
        send(gate_out.at[slot], gate_in.at[x], ass.at[n], asr.at[n], device)
    gate_in[x] = gate_out[x]

    w_1(0)
    w_1(1)
    o_arrive(0, x_l, 0, 128)
    o_send(2, x_l, 0, 64, right)
    o_arrive(1, x_r, 0, 128)
    o_send(3, x_r, 64, 64, left)
    for n, slot in ((4, x_l), (5, x_r)):
        o_send(n, slot, 0, 128, sibling)
    w_pass_on(0, 0)
    w_pass_on(1, 0)
    o_arrive(2, x_a, 0, 64)
    o_arrive(3, x_a, 64, 64)
    o_send(6, x_a, 0, 128, sibling)
    for n, slot in enumerate((x_l, x_r, x_a)):
        arrive(gate_in.at[slot], ass.at[n], asr.at[n])
    for n, slot in enumerate((x_l, x_r, x_a)):
        arrive(ow.at[slot, pl.ds((1 - c) * 128, 128)], oss.at[4 + n], osr.at[4 + n])

    in_res.wait()

    def project(n, squares):
        cols = pl.ds(pl.multiple_of(n * 256, 256), 256)
        acc = res[:, cols].astype(F32)
        acc = acc + (
            (dot(gate_in[0], ow[0, :, cols]) + dot(gate_in[1], ow[1, :, cols]))
            + (dot(gate_in[2], ow[2, :, cols]) + dot(gate_in[3], ow[3, :, cols]))
        )
        stream[:, cols] = acc
        return squares + (acc[:, :128] * acc[:, :128] + acc[:, 128:] * acc[:, 128:])

    squares = lax.fori_loop(0, D // 256, project, jnp.zeros((R, 128), F32))
    inverse = lax.rsqrt(jnp.sum(squares, axis=1, keepdims=True) / D + NORM_EPS)

    def normalize(n, carry):
        cols = pl.ds(pl.multiple_of(n * 256, 256), 256)
        gain_row = jnp.concatenate([gsc[pl.ds(2 * n, 1), :], gsc[pl.ds(2 * n + 1, 1), :]], axis=1)
        rows[x, :, cols] = (stream[:, cols] * inverse * gain_row).astype(BF)
        return carry

    lax.fori_loop(0, D // 256, normalize, 0)

    def r_at(slot, half):
        return rows.at[slot, pl.ds(128 * half, 128)]

    def r_send(n, slot, half, device):
        send(r_at(slot, half), r_at(slot, half), gss.at[n], gsr.at[n], device)

    def r_arrive(n, slot, half):
        arrive(r_at(slot, half), gss.at[n], gsr.at[n])

    r_send(0, x, 0, right)
    r_send(1, x, 1, left)
    r_send(2, x, 1, right)
    r_send(3, x, 0, left)

    w_2(0)
    w_2(1)
    for n in (1, 2):
        w_pass_on(0, n)
        w_pass_on(1, n)
    w_finish(0, 0)
    w_finish(1, 0)
    r_arrive(0, x_l, 0)
    r_send(4, x_l, 0, right)
    r_arrive(1, x_r, 1)
    r_send(5, x_r, 1, left)
    w_pass_on(0, 3)
    w_pass_on(1, 3)
    for n in (1, 2, 3):
        w_finish(0, n)
        w_finish(1, n)
    for n in range(4):
        w_line(0, n, True)
        w_line(1, n, True)

    up_half, low_half = pl.ds(0, 128), pl.ds(128, 128)

    def widen(n, pieces):
        def one(j, carry):
            both = jnp.concatenate(
                [w[2 * j].reshape(D, 128), w[2 * j + 1].reshape(D, 128)], axis=1
            )
            acts = dot(jnp.concatenate([rows[piece] for piece in pieces], axis=0), both)
            gate_act, up_act = acts[:, :128], acts[:, 128:]
            cols = pl.ds(pl.multiple_of(j * 128, 128), 128)
            hid[n, :, cols] = (gate_act * (1.0 / (1.0 + jnp.exp(-gate_act))) * up_act).astype(BF)
            return carry

        lax.fori_loop(0, NJ, one, 0)

    def narrow(n, store, first=0, last=D // 256):
        def one(t, carry):
            down = jnp.concatenate(
                [
                    w[2 * NJ + j, t // 2, pl.ds(2 * lax.rem(t, 2), 2)].reshape(256, 128)
                    for j in range(NJ)
                ],
                axis=1,
            )
            store(pl.ds(pl.multiple_of(t * 256, 256), 256), dot_nt(hid[n], down))
            return carry

        lax.fori_loop(first, last, one, 0)

    def keep(n):
        def store(cols, value):
            part[n, :, cols] = value.astype(BF)

        return store

    def p_send(n, src, dst, device):
        send(src, dst, rss.at[n], rsr.at[n], device)

    def p_arrive(n, ref):
        arrive(ref, rss.at[n], rsr.at[n])

    def piece(ref, slot, half, side):
        return ref.at[slot, half, pl.ds(1024 * side, 1024)]

    widen(0, ((x_l, up_half), (x_r, low_half)))
    narrow(0, keep(0))
    p_send(0, part.at[0, low_half], fin.at[0, low_half], right)
    p_send(1, part.at[0, up_half], fin.at[1, up_half], left)
    r_arrive(2, x_l, 1)
    r_arrive(3, x_r, 0)
    widen(1, ((x_r, up_half), (x_l, low_half)))
    r_arrive(4, x_a, 0)
    r_arrive(5, x_a, 1)
    widen(2, ((x_a, up_half), (x_a, low_half)))
    for side in range(2):
        narrow(2, keep(2), 4 * side, 4 * side + 4)
        p_send(2 + 2 * side, piece(part, 2, up_half, side), piece(mid, 0, up_half, side), right)
        p_send(3 + 2 * side, piece(part, 2, low_half, side), piece(mid, 1, up_half, side), left)
    narrow(1, keep(1))
    widen(3, ((x, up_half), (x, low_half)))
    for side in range(2):
        at = pl.ds(1024 * side, 1024)
        p_arrive(2 + 2 * side, piece(mid, 0, up_half, side))
        part[1, up_half, at] = (part[1, up_half, at].astype(F32) + mid[0, :, at].astype(F32)).astype(BF)
        p_send(6 + 2 * side, piece(part, 1, up_half, side), piece(fin, 0, up_half, side), right)
        p_arrive(3 + 2 * side, piece(mid, 1, up_half, side))
        part[1, low_half, at] = (part[1, low_half, at].astype(F32) + mid[1, :, at].astype(F32)).astype(BF)
        p_send(7 + 2 * side, piece(part, 1, low_half, side), piece(fin, 1, low_half, side), left)
    def own(cols, value):
        stream[:, cols] = stream[:, cols] + 0.5 * value

    narrow(3, own)
    p_arrive(0, fin.at[0, low_half])
    p_arrive(1, fin.at[1, up_half])
    for side in range(2):
        p_arrive(6 + 2 * side, piece(fin, 0, up_half, side))
        p_arrive(7 + 2 * side, piece(fin, 1, low_half, side))

    def finish(n, carry):
        cols = pl.ds(pl.multiple_of(n * 256, 256), 256)
        others = fin[0, :, cols].astype(F32) + fin[1, :, cols].astype(F32)
        out[:, cols] = (stream[:, cols] + 0.5 * others).astype(BF)
        return carry

    lax.fori_loop(0, D // 256, finish, 0)
    for copy in sent:
        copy.wait_send()


def body(
    query_rows,
    key_rows,
    value_rows,
    input_gate,
    forget_gate,
    output_gate,
    documents,
    residual,
    out_weight,
    norm_gain,
    gate_weight,
    up_weight,
    down_weight,
):
    vmem = pl.BlockSpec(memory_space=pltpu.VMEM)
    hbm = pl.BlockSpec(memory_space=pl.ANY)
    dma = pltpu.SemaphoreType.DMA
    return pl.pallas_call(
        kernel,
        out_shape=jax.ShapeDtypeStruct((R, D), BF),
        in_specs=[vmem] * 4 + [hbm] * 9,
        out_specs=vmem,
        scratch_shapes=[
            pltpu.VMEM((T, 256), BF),
            pltpu.VMEM((T, 256), BF),
            pltpu.VMEM((T, 256), BF),
            pltpu.VMEM((T, 256), BF),
            pltpu.VMEM((R, D), BF),
            pltpu.VMEM((64, FD), BF),
            pltpu.VMEM((64, FD), BF),
            pltpu.VMEM((64, FD), BF),
            pltpu.VMEM((TILES, 4, 4, 2, 64, 128), BF),
            pltpu.VMEM((4, 256, D), BF),
            pltpu.VMEM((264, 128), F32),
            pltpu.VMEM((264, 128), F32),
            pltpu.VMEM((256, 128), BF),
            pltpu.VMEM((8, 128), F32),
            pltpu.VMEM((LOOK, 256, 128), BF),
            pltpu.VMEM((LOOK, 8, 128), F32),
            pltpu.VMEM((4, R, 256), BF),
            pltpu.VMEM((4, R, 256), BF),
            pltpu.VMEM((R, D), F32),
            pltpu.VMEM((4, R, D), BF),
            pltpu.VMEM((4, R, FD), BF),
            pltpu.VMEM((3, R, D), BF),
            pltpu.VMEM((2, 128, D), BF),
            pltpu.VMEM((2, R, D), BF),
            pltpu.VMEM((128, 128), F32),
            pltpu.VMEM((128, 128), F32),
            pltpu.VMEM((16, 128), F32),
            pltpu.VMEM((8, 128), F32),
            pltpu.VMEM((16, 128), F32),
            pltpu.VMEM((2, T, 256), BF),
            pltpu.VMEM((2, T, 256), F32),
            pltpu.VMEM((T, 256), F32),
            dma((9,)),
            dma((2, 24)),
            dma((2, 24)),
            dma((7,)),
            dma((7,)),
            dma((2 * LOOK + 1,)),
            dma((2 * LOOK + 1,)),
            dma((3,)),
            dma((3,)),
            dma((6,)),
            dma((6,)),
            dma((10,)),
            dma((10,)),
        ],
        compiler_params=pltpu.CompilerParams(
            collective_id=0, has_side_effects=True, vmem_limit_bytes=62 * 1024 * 1024
        ),
    )(
        input_gate,
        forget_gate,
        documents.reshape(8, 128),
        norm_gain.reshape(16, 128),
        query_rows,
        key_rows,
        value_rows,
        output_gate,
        residual,
        out_weight,
        gate_weight,
        up_weight,
        down_weight.T,
    )


def solution(mesh):
    torus = Mesh(mesh.devices.reshape(4, 4, 2, mesh.shape["tp"]), SP_TP)
    in_specs = (
        P(SP, "tp"),
        P(SP, "tp"),
        P(SP, "tp"),
        P("tp", SP),
        P("tp", SP),
        P(SP, "tp"),
        P(SP),
        P(SP_TP, None),
        P("tp", None),
        P(),
        P(SP, "tp"),
        P(SP, "tp"),
        P("tp", SP),
    )
    out_specs = P(SP_TP, None)
    return jax.shard_map(body, mesh=torus, in_specs=in_specs, out_specs=out_specs, check_vma=False)
```

```python
import jax
import jax.numpy as jnp
from jax import lax
from jax.experimental import pallas as pl
from jax.experimental.pallas import tpu as pltpu
from jax.sharding import Mesh
from jax.sharding import PartitionSpec as P

HD = 128
SP = ("sp_0", "sp_1", "sp_2")
SP_TP = ("sp_0", "sp_1", "sp_2", "tp")
MESH = pl.DeviceIdType.MESH
BF = jnp.bfloat16
F32 = jnp.float32

NORM_EPS = 1e-06
NEG = -1e30
T = 1024
R = 256
D = 2048
FD = 1408
NJ = FD // 128
LOOK = 3
TILES = 3 * NJ
PARTS = ((0, 9, 5), (9, 13, 6), (22, 5, 3), (27, 6, 3))


def dot(a, b):
    return jnp.dot(a, b, preferred_element_type=F32)


def dot_nt(a, b):
    return lax.dot_general(a, b, (((1,), (1,)), ((), ())), preferred_element_type=F32)


def dot_tn(a, b):
    return lax.dot_general(a, b, (((0,), (0,)), ((), ())), preferred_element_type=F32)


def split(a):
    hi = a.astype(BF)
    return hi, (a - hi.astype(F32)).astype(BF)


def kernel(
    in_gate_hbm,
    forget_hbm,
    doc_hbm,
    gain_hbm,
    q_hbm,
    k_hbm,
    v_hbm,
    og_hbm,
    res_hbm,
    ow_hbm,
    wg_hbm,
    wu_hbm,
    wd_hbm,
    out,
    in_gate,
    forget,
    doc_ref,
    gain,
    q,
    k,
    v,
    og,
    res,
    wg,
    wu,
    wd,
    w,
    ow,
    st_out,
    st_twin,
    mem_out,
    meta_out,
    mem_in,
    meta_in,
    gate_out,
    gate_in,
    gate_relay,
    stream,
    rows,
    hid,
    part,
    mid,
    fin,
    vt,
    tt,
    arow,
    drow,
    gsc,
    vones,
    numden,
    opened,
    lsem,
    wss,
    wsr,
    oss,
    osr,
    sss,
    ssr,
    ass,
    asr,
    gss,
    gsr,
    rss,
    rsr,
):
    z, y, c, x = (lax.axis_index(n) for n in SP_TP)

    def step(a, by):
        return lax.rem(a + by + 8, 4)

    chip = z * 4 + y

    def chip_ahead(by):
        i = lax.rem(chip + by + 16, 16)
        return {"sp_0": i // 4, "sp_1": lax.rem(i, 4)}

    sibling = {"sp_2": 1 - c}
    peers = [sibling]
    for name, at in (("sp_0", z), ("sp_1", y), ("tp", x)):
        peers += [{name: step(at, 1)}, {name: step(at, -1)}]
    peers += [{"tp": step(x, 2)}]
    for d in range(1, LOOK + 1):
        peers += [chip_ahead(d), chip_ahead(-d)]

    barrier = pltpu.get_barrier_semaphore()
    for peer in peers:
        pl.semaphore_signal(barrier, inc=1, device_id=peer, device_id_type=MESH)

    local = []
    for n, (src, dst) in enumerate(
        (
            (in_gate_hbm, in_gate),
            (forget_hbm, forget),
            (doc_hbm, doc_ref),
            (gain_hbm, gain),
            (ow_hbm, ow.at[x]),
            (wg_hbm, wg),
            (wu_hbm, wu),
            (wd_hbm, wd),
            (k_hbm, k),
            (v_hbm, v),
            (q_hbm, q),
            (og_hbm, og),
            (res_hbm, res),
        )
    ):
        copy = pltpu.make_async_copy(src, dst, lsem.at[n])
        copy.start()
        local.append(copy)
    small, (in_ow, in_wg, in_wu, in_wd, in_k, in_v, in_q, in_og, in_res) = local[:4], local[4:]

    sent = []

    def remote(src, dst, send_sem, recv_sem, device):
        return pltpu.make_async_remote_copy(
            src_ref=src,
            dst_ref=dst,
            send_sem=send_sem,
            recv_sem=recv_sem,
            device_id=device,
            device_id_type=MESH,
        )

    def send(*args):
        copy = remote(*args)
        copy.start()
        sent.append(copy)

    def arrive(ref, send_sem, recv_sem):
        remote(ref, ref, send_sem, recv_sem, sibling).wait_recv()

    def w_axes(p):
        return (("sp_0", z), ("sp_1", y)) if p % 2 == 0 else (("sp_1", y), ("sp_0", z))

    def w_at(p, first, count, uu, vv):
        zz, yy = (uu, vv) if p % 2 == 0 else (vv, uu)
        return w.at[pl.ds(first, count), zz, yy, c]

    def w_send(p, n, first, count, uu, vv, device):
        ref = w_at(p, first, count, uu, vv)
        send(ref, ref, wss.at[p, n], wsr.at[p, n], device)

    def w_arrive(p, n, first, count, uu, vv):
        arrive(w_at(p, first, count, uu, vv), wss.at[p, n], wsr.at[p, n])

    LINE = (0, -1, 1, 2)

    def w_spread(p, n):
        (_, uu), (vn, vv) = w_axes(p)
        first, count, _ = PARTS[p]
        for s, by in ((0, 1), (1, -1)):
            w_send(p, 4 + 4 * n + s, first, count, step(uu, LINE[n]), vv, {vn: step(vv, by)})

    def w_pass_on(p, n):
        (_, uu), (vn, vv) = w_axes(p)
        first, count, half = PARTS[p]
        k_at = step(uu, LINE[n])
        w_arrive(p, 4 + 4 * n, first, count, k_at, step(vv, -1))
        w_send(p, 6 + 4 * n, first, half, k_at, step(vv, -1), {vn: step(vv, 1)})
        w_arrive(p, 5 + 4 * n, first, count, k_at, step(vv, 1))
        w_send(p, 7 + 4 * n, first + half, count - half, k_at, step(vv, 1), {vn: step(vv, -1)})

    def w_line(p, n, get):
        (_, uu), _ = w_axes(p)
        first, count, _ = PARTS[p]
        k_at = step(uu, LINE[n])
        core = 1 - c if get else c
        span = pl.ds(first, count)
        ref = w.at[span, k_at, :, core] if p % 2 == 0 else w.at[span, :, k_at, core]
        if get:
            arrive(ref, wss.at[p, 20 + n], wsr.at[p, 20 + n])
        else:
            send(ref, ref, wss.at[p, 20 + n], wsr.at[p, 20 + n], sibling)

    def w_finish(p, n):
        (_, uu), (_, vv) = w_axes(p)
        first, count, half = PARTS[p]
        k_at = step(uu, LINE[n])
        w_arrive(p, 6 + 4 * n, first, half, k_at, step(vv, 2))
        w_arrive(p, 7 + 4 * n, first + half, count - half, k_at, step(vv, 2))
        w_line(p, n, False)

    def w_0(name):
        for p in (0, 1, 2, 3) if name == "sp_0" else (1, 0, 3, 2):
            (un, uu), (_, vv) = w_axes(p)
            first, count, _ = PARTS[p]
            if un == name:
                for n, by in ((0, 1), (1, -1)):
                    w_send(p, n, first, count, uu, vv, {un: step(uu, by)})
            else:
                w_spread(p, 0)

    def w_1(p):
        (un, uu), (_, vv) = w_axes(p)
        first, count, half = PARTS[p]
        w_arrive(p, 0, first, count, step(uu, -1), vv)
        w_send(p, 2, first, half, step(uu, -1), vv, {un: step(uu, 1)})
        w_spread(p, 1)
        w_arrive(p, 1, first, count, step(uu, 1), vv)
        w_send(p, 3, first + half, count - half, step(uu, 1), vv, {un: step(uu, -1)})
        w_spread(p, 2)

    def w_2(p):
        (_, uu), (_, vv) = w_axes(p)
        first, count, half = PARTS[p]
        w_arrive(p, 2, first, half, step(uu, 2), vv)
        w_arrive(p, 3, first + half, count - half, step(uu, 2), vv)
        w_spread(p, 3)

    right, left, across = {"tp": step(x, 1)}, {"tp": step(x, -1)}, {"tp": step(x, 2)}
    x_r, x_l, x_a = step(x, 1), step(x, -1), step(x, 2)

    def o_at(slot, part_first, count):
        return ow.at[slot, pl.ds(c * 128 + part_first, count)]

    def o_send(n, slot, first, count, device):
        send(o_at(slot, first, count), o_at(slot, first, count), oss.at[n], osr.at[n], device)


    def o_arrive(n, slot, first, count):
        arrive(o_at(slot, first, count), oss.at[n], osr.at[n])

    pl.semaphore_wait(barrier, len(peers))
    in_ow.wait()
    o_send(0, x, 0, 64, right)
    o_send(1, x, 64, 64, left)
    o_send(2, x, 64, 64, right)
    o_send(3, x, 0, 64, left)

    in_wg.wait()
    in_wu.wait()
    in_wd.wait()
    for j in range(NJ):
        cols = slice(128 * j, 128 * j + 128)
        w[2 * j, z, y, c] = wg[:, cols]
        w[2 * j + 1, z, y, c] = wu[:, cols]
        w[2 * NJ + j, z, y, c] = wd[:, cols]

    w_0("sp_0")

    for copy in small:
        copy.wait()
    lane = lax.broadcasted_iota(jnp.int32, (8, 128), 1)
    row = lax.broadcasted_iota(jnp.int32, (8, 128), 0)
    docs = doc_ref[...].astype(F32)
    drow[...] = docs
    gsc[...] = gain[...].astype(F32)
    last_lane = jnp.broadcast_to(docs[:, 127:128], (8, 128))
    heads = []
    vt[...] = jnp.zeros_like(vt)

    def eight_rows(ref, h):
        return jnp.concatenate([ref[h : h + 1, 128 * n : 128 * n + 128] for n in range(8)], axis=0)

    for h in range(2):
        cum = eight_rows(forget, h)
        cum = jnp.minimum(cum, 0.0) - jnp.log1p(jnp.exp(-jnp.abs(cum)))
        for s in (1, 2, 4, 8, 16, 32, 64):
            cum = cum + jnp.where(lane >= s, pltpu.roll(cum, s, 1), 0.0)
        upto = jnp.broadcast_to(cum[:, 127:128], (8, 128))
        for s in (1, 2, 4):
            upto = upto + jnp.where(row >= s, pltpu.roll(upto, s, 0), 0.0)
        cum = cum + jnp.where(row >= 1, pltpu.roll(upto, 1, 0), 0.0)
        a = eight_rows(in_gate, h) - cum
        m = a
        for s in (1, 2, 4, 8, 16, 32, 64):
            ok = (lane >= s) & (pltpu.roll(docs, s, 1) == docs)
            m = jnp.where(ok, jnp.maximum(m, pltpu.roll(m, s, 1)), m)
        e = jnp.broadcast_to(m[:, 127:128], (8, 128))
        for s in (1, 2, 4):
            ok = (row >= s) & (pltpu.roll(last_lane, s, 0) == last_lane)
            e = jnp.where(ok, jnp.maximum(e, pltpu.roll(e, s, 0)), e)
        ok = (row >= 1) & (pltpu.roll(last_lane, 1, 0) == docs)
        m = jnp.where(ok, jnp.maximum(m, pltpu.roll(e, 1, 0)), m)
        top = e[7:8, :]
        last = last_lane[7:8, :]
        weight = jnp.where(docs == last, jnp.exp(a - top), 0.0)
        arow[8 * h : 8 * h + 8, :] = a
        vt[8 * h : 8 * h + 8, :] = m
        vt[16 + 8 * h : 24 + 8 * h, :] = weight
        total = upto[7:8, :]
        heads.append((top + total, total, m))
    vt[32:40, :] = docs
    tt[...] = vt[...].T

    in_k.wait()
    in_v.wait()
    normers = []
    for h in range(2):
        cols = slice(h * HD, h * HD + HD)
        kw = jnp.concatenate(
            [
                k[128 * n : 128 * n + 128, cols].astype(F32)
                * tt[:, 16 + 8 * h + n : 17 + 8 * h + n]
                for n in range(8)
            ],
            axis=0,
        )
        hi, lo = split(kw)
        st_out[HD * h : HD * h + HD, :] = dot_tn(hi, v[:, cols]) + dot_tn(lo, v[:, cols])
        normers.append(jnp.sum(kw, axis=0, keepdims=True))
    st_out[256:264, :] = jnp.concatenate(
        normers
        + [heads[0][0], heads[1][0], heads[0][1], heads[1][1], last, last],
        axis=0,
    )

    send(st_out, st_twin, sss.at[0], ssr.at[0], sibling)

    arrive(st_twin, sss.at[0], ssr.at[0])
    first_core = c == 0
    mine, twin = st_out[256:264, :], st_twin[256:264, :]
    early = jnp.where(first_core, mine, twin)
    late = jnp.where(first_core, twin, mine)
    goes = early[6:7, :] == late[6:7, :]
    meta = [None] * 8
    for h in range(2):
        span = slice(HD * h, HD * h + HD)
        one = jnp.where(goes, early[2 + h : 3 + h, :] + late[4 + h : 5 + h, :], NEG)
        two = late[2 + h : 3 + h, :]
        stab = jnp.maximum(one, two)
        share_one = jnp.where(goes, jnp.exp(one - stab), 0.0)
        share_two = jnp.exp(two - stab)
        share_mine = jnp.where(first_core, share_one, share_two)
        share_twin = jnp.where(first_core, share_two, share_one)
        mem_out[span, :] = (share_mine * st_out[span, :] + share_twin * st_twin[span, :]).astype(BF)
        meta[h] = share_mine * mine[h : h + 1, :] + share_twin * twin[h : h + 1, :]
        meta[2 + h] = stab
        meta[4 + h] = early[4 + h : 5 + h, :] + late[4 + h : 5 + h, :]
    meta[6] = meta[7] = late[6:7, :]
    meta_out[...] = jnp.concatenate(meta, axis=0)
    head = pl.ds(HD * c, HD)
    for d in range(1, LOOK + 1):
        send(meta_out, meta_in.at[d - 1], sss.at[2 * d], ssr.at[2 * d], chip_ahead(d))
        send(mem_out.at[head], mem_in.at[d - 1, head], sss.at[2 * d - 1], ssr.at[2 * d - 1], chip_ahead(d))

    w_0("sp_1")

    in_q.wait()
    for h in range(2):
        vones[h, :, :HD] = v[:, HD * h : HD * h + HD]
        vones[h, :, HD:] = jnp.ones((T, HD), BF)

    def column(n):
        return jnp.concatenate([tt[:, n : n + 1], tt[:, n + 1 : n + 2]], axis=0)

    for h in range(2):
        cols = slice(h * HD, h * HD + HD)
        for i in range(4):
            at = slice(256 * i, 256 * i + 256)
            m_col, d_col = column(8 * h + 2 * i), column(32 + 2 * i)
            acc = jnp.zeros((256, 2 * HD), F32)
            for j in range(i + 1):
                keys = slice(256 * j, 256 * j + 256)
                a_row, d_row = (
                    jnp.concatenate([ref[n + 2 * j : n + 2 * j + 1, :], ref[n + 2 * j + 1 : n + 2 * j + 2, :]], axis=1)
                    for ref, n in ((arow, 8 * h), (drow, 0))
                )
                ok = d_col == d_row
                if i == j:
                    ok = ok & (
                        lax.broadcasted_iota(jnp.int32, (256, 256), 0)
                        >= lax.broadcasted_iota(jnp.int32, (256, 256), 1)
                    )
                p = jnp.where(ok, dot_nt(q[at, cols], k[keys, cols]) * jnp.exp(a_row - m_col), 0.0)
                hi, lo = split(p)
                acc = acc + (dot(hi, vones[h, keys, :]) + dot(lo, vones[h, keys, :]))
            numden[h, at, :] = acc
    in_og.wait()
    for i in range(4):
        at = slice(256 * i, 256 * i + 256)
        opened[at, :] = 1.0 / (1.0 + jnp.exp(-og[at, :].astype(F32)))

    o_arrive(0, x_l, 0, 64)
    o_send(4, x_l, 0, 64, right)
    o_arrive(1, x_r, 64, 64)
    o_send(5, x_r, 64, 64, left)
    for d in range(1, LOOK + 1):
        arrive(mem_in.at[d - 1, head], sss.at[2 * d - 1], ssr.at[2 * d - 1])
        n = 2 * LOOK + d
        send(mem_in.at[d - 1, head], mem_in.at[d - 1, head], sss.at[n], ssr.at[n], sibling)
    for d in range(1, LOOK + 1):
        n = 2 * LOOK + d
        arrive(meta_in.at[d - 1], sss.at[2 * d], ssr.at[2 * d])
        arrive(mem_in.at[d - 1, pl.ds(HD * (1 - c), HD)], sss.at[n], ssr.at[n])
    second_core = c == 1
    one_back = meta_in[0, 6:7, :]
    carry_doc = jnp.where(second_core, twin[6:7, :], jnp.where(chip > 0, one_back, -1.0))
    scale = HD**-0.5
    memories = []
    for h in range(2):
        passed = jnp.where(second_core, twin[4 + h : 5 + h, :], 0.0)
        levels = [jnp.where(second_core, twin[2 + h : 3 + h, :], NEG)]
        for d in range(1, LOOK + 1):
            ok = (meta_in[d - 1, 6:7, :] == carry_doc) & (chip >= d)
            levels.append(jnp.where(ok, meta_in[d - 1, 2 + h : 3 + h, :] + passed, NEG))
            passed = passed + meta_in[d - 1, 4 + h : 5 + h, :]
        stab = levels[0]
        for level in levels[1:]:
            stab = jnp.maximum(stab, level)
        shares = [jnp.where(level > 0.5 * NEG, jnp.exp(level - stab), 0.0) for level in levels]
        memory = shares[0] * st_twin[HD * h : HD * h + HD, :]
        normer = shares[0] * twin[h : h + 1, :]
        for d in range(1, LOOK + 1):
            memory = memory + shares[d] * mem_in[d - 1, HD * h : HD * h + HD, :].astype(F32)
            normer = normer + shares[d] * meta_in[d - 1, h : h + 1, :]
        memories.append(memory)
        m = heads[h][2]
        goes_on = docs == carry_doc
        both = jnp.where(goes_on, jnp.maximum(m, stab), m)
        vt[8 * h : 8 * h + 8, :] = jnp.exp(m - both) * scale
        vt[16 + 8 * h : 24 + 8 * h, :] = jnp.where(goes_on, jnp.exp(stab - both), 0.0) * scale
        vt[32 + 8 * h : 40 + 8 * h, :] = jnp.broadcast_to(normer, (8, HD))
    tt[...] = vt[...].T
    for h in range(2):
        cols = slice(h * HD, h * HD + HD)
        normer = jnp.broadcast_to(tt[:, 32 + 8 * h : 33 + 8 * h], (HD, HD))
        parts = [jnp.concatenate(pair, axis=1) for pair in zip(split(memories[h]), split(normer))]
        for i in range(4):
            at = slice(256 * i, 256 * i + 256)
            scale_in, scale_by = column(8 * h + 2 * i), column(16 + 8 * h + 2 * i)
            queries = q[at, cols]
            both = scale_in * numden[h, at, :] + scale_by * (dot(queries, parts[0]) + dot(queries, parts[1]))
            cell = both[:, :HD] / jnp.maximum(jnp.abs(both[:, HD:]), 1.0)
            gate_out[i, :, cols] = (cell * opened[at, cols]).astype(BF)

    def half_of(ref, slot, half):
        return ref.at[slot, pl.ds(128 * half, 128)]

    onward, behind = {"tp": lax.rem(x + 1 + 2 * c, 4)}, lax.rem(x + 3 + 2 * c, 4)

    def g_send(n, half, src, dst, device):
        m = 4 * half + n
        send(half_of(*src, half), half_of(*dst, half), ass.at[m], asr.at[m], device)

    def g_arrive(n, half, ref, slot):
        m = 4 * half + n
        arrive(half_of(ref, slot, half), ass.at[m], asr.at[m])

    for half in range(2):
        g_send(2, half, (gate_out, x_a), (gate_relay, 0), onward)
    for half in range(2):
        g_send(0, half, (gate_out, x_r), (gate_in, x), right)
        g_send(1, half, (gate_out, x_l), (gate_in, x), left)

    def relay(half):
        g_arrive(2, half, gate_relay, 0)
        g_send(3, half, (gate_relay, 0), (gate_in, behind), onward)

    gate_in[x] = gate_out[x]

    w_1(0)
    w_pass_on(1, 0)
    w_1(1)
    w_pass_on(0, 0)
    o_arrive(2, x_l, 64, 64)
    o_arrive(3, x_r, 0, 64)
    for n, slot in ((6, x_l), (7, x_r)):
        o_send(n, slot, 0, 128, sibling)
    w_1(2)
    w_pass_on(3, 0)
    w_1(3)
    w_pass_on(2, 0)
    o_arrive(4, x_a, 0, 64)
    o_arrive(5, x_a, 64, 64)
    o_send(8, x_a, 0, 128, sibling)
    relay(0)
    relay(1)
    for n, slot in enumerate((x_l, x_r, x_a)):
        arrive(ow.at[slot, pl.ds((1 - c) * 128, 128)], oss.at[6 + n], osr.at[6 + n])
    in_res.wait()

    def output_rows(half):
        span = pl.ds(128 * half, 128)

        def project(n, squares):
            cols = pl.ds(pl.multiple_of(n * 256, 256), 256)
            cells = jnp.concatenate([gate_in[n, span] for n in range(4)], axis=1)
            acc = res[span, cols].astype(F32) + dot(cells, ow[:, :, cols].reshape(1024, 256))
            stream[span, cols] = acc
            return squares + (acc[:, :128] * acc[:, :128] + acc[:, 128:] * acc[:, 128:])

        squares = lax.fori_loop(0, D // 256, project, jnp.zeros((128, 128), F32))
        inverse = lax.rsqrt(jnp.sum(squares, axis=1, keepdims=True) / D + NORM_EPS)

        def normalize(n, carry):
            cols = pl.ds(pl.multiple_of(n * 256, 256), 256)
            gain_row = jnp.concatenate([gsc[pl.ds(2 * n, 1), :], gsc[pl.ds(2 * n + 1, 1), :]], axis=1)
            rows[x, span, cols] = (stream[span, cols] * inverse * gain_row).astype(BF)
            return carry

        lax.fori_loop(0, D // 256, normalize, 0)

    def r_at(slot, first, count):
        return rows.at[slot, pl.ds(first, count)]

    def r_send(n, slot, first, count, device):
        send(r_at(slot, first, count), r_at(slot, first, count), gss.at[n], gsr.at[n], device)

    def r_arrive(n, slot, first, count):
        arrive(r_at(slot, first, count), gss.at[n], gsr.at[n])

    def gated_rows(half):
        for n, slot in ((0, x_l), (1, x_r), (3, x_a)):
            g_arrive(n, half, gate_in, slot)

    gated_rows(0)
    output_rows(0)
    r_send(0, x, 0, 128, right)
    r_send(1, x, 0, 128, left)
    gated_rows(1)
    output_rows(1)
    r_send(2, x, 128, 128, right)
    r_send(3, x, 128, 64, left)
    r_send(4, x, 192, 64, left)

    w_2(0)
    w_2(1)
    for n in (1, 2):
        w_pass_on(0, n)
        w_pass_on(1, n)
    w_finish(0, 0)
    w_finish(1, 0)
    w_2(2)
    w_2(3)
    w_pass_on(1, 3)
    w_pass_on(0, 3)
    for n in (1, 2):
        w_pass_on(2, n)
        w_pass_on(3, n)
    r_arrive(0, x_l, 0, 128)
    r_send(5, x_l, 0, 128, right)
    for n in (1, 2):
        w_finish(0, n)
        w_finish(1, n)
    w_pass_on(3, 3)
    w_pass_on(2, 3)
    w_finish(0, 3)
    w_finish(1, 3)
    for n in (0, 1, 2):
        w_finish(2, n)
        w_finish(3, n)
    r_arrive(3, x_r, 128, 64)
    r_send(6, x_r, 128, 64, left)
    r_arrive(4, x_r, 192, 64)
    r_send(7, x_r, 192, 64, left)
    w_finish(2, 3)
    w_finish(3, 3)
    for n in range(4):
        w_line(0, n, True)
        w_line(1, n, True)

    up_half, low_half = pl.ds(0, 128), pl.ds(128, 128)

    def widen(n, pieces):
        def one(j, carry):
            both = jnp.concatenate(
                [w[2 * j].reshape(D, 128), w[2 * j + 1].reshape(D, 128)], axis=1
            )
            acts = dot(jnp.concatenate([rows[piece] for piece in pieces], axis=0), both)
            gate_act, up_act = acts[:, :128], acts[:, 128:]
            cols = pl.ds(pl.multiple_of(j * 128, 128), 128)
            hid[n, :, cols] = (gate_act * (1.0 / (1.0 + jnp.exp(-gate_act))) * up_act).astype(BF)
            return carry

        lax.fori_loop(0, NJ, one, 0)

    def narrow(n, store, first=0, last=D // 256):
        def one(t, carry):
            down = jnp.concatenate(
                [
                    w[2 * NJ + j, t // 2, pl.ds(2 * lax.rem(t, 2), 2)].reshape(256, 128)
                    for j in range(NJ)
                ],
                axis=1,
            )
            store(pl.ds(pl.multiple_of(t * 256, 256), 256), dot_nt(hid[n], down))
            return carry

        lax.fori_loop(first, last, one, 0)

    def keep(n):
        def store(cols, value):
            part[n, :, cols] = value.astype(BF)

        return store

    def p_send(n, src, dst, device):
        send(src, dst, rss.at[n], rsr.at[n], device)

    def p_arrive(n, ref):
        arrive(ref, rss.at[n], rsr.at[n])

    def piece(ref, slot, half, side):
        return ref.at[slot, half, pl.ds(1024 * side, 1024)]

    widen(0, ((x_l, up_half), (x_r, low_half)))
    for n in range(4):
        w_line(2, n, True)
        w_line(3, n, True)
    for side in range(2):
        narrow(0, keep(0), 4 * side, 4 * side + 4)
        p_send(10 * side, piece(part, 0, low_half, side), piece(fin, 0, low_half, side), right)
        p_send(10 * side + 1, piece(part, 0, up_half, side), piece(fin, 1, up_half, side), left)
    r_arrive(5, x_a, 0, 128)
    r_arrive(6, x_a, 128, 64)
    r_arrive(7, x_a, 192, 64)
    widen(2, ((x_a, up_half), (x_a, low_half)))
    for side in range(2):
        narrow(2, keep(2), 4 * side, 4 * side + 4)
        p_send(2 + 2 * side, piece(part, 2, up_half, side), piece(mid, 0, up_half, side), right)
        p_send(3 + 2 * side, piece(part, 2, low_half, side), piece(mid, 1, up_half, side), left)
    r_arrive(2, x_l, 128, 128)
    r_arrive(1, x_r, 0, 128)
    widen(1, ((x_r, up_half), (x_l, low_half)))
    narrow(1, keep(1))

    def pass_sum(side):
        at = pl.ds(1024 * side, 1024)
        p_arrive(2 + 2 * side, piece(mid, 0, up_half, side))
        part[1, up_half, at] = (part[1, up_half, at].astype(F32) + mid[0, :, at].astype(F32)).astype(BF)
        p_send(6 + 2 * side, piece(part, 1, up_half, side), piece(fin, 0, up_half, side), right)
        p_arrive(3 + 2 * side, piece(mid, 1, up_half, side))
        part[1, low_half, at] = (part[1, low_half, at].astype(F32) + mid[1, :, at].astype(F32)).astype(BF)
        p_send(7 + 2 * side, piece(part, 1, low_half, side), piece(fin, 1, low_half, side), left)

    pass_sum(0)
    widen(3, ((x, up_half), (x, low_half)))
    pass_sum(1)
    def own(cols, value):
        stream[:, cols] = stream[:, cols] + 0.5 * value

    narrow(3, own)
    for side in range(2):
        p_arrive(10 * side, piece(fin, 0, low_half, side))
        p_arrive(10 * side + 1, piece(fin, 1, up_half, side))
        p_arrive(6 + 2 * side, piece(fin, 0, up_half, side))
        p_arrive(7 + 2 * side, piece(fin, 1, low_half, side))

    def finish(n, carry):
        cols = pl.ds(pl.multiple_of(n * 256, 256), 256)
        others = fin[0, :, cols].astype(F32) + fin[1, :, cols].astype(F32)
        out[:, cols] = (stream[:, cols] + 0.5 * others).astype(BF)
        return carry

    lax.fori_loop(0, D // 256, finish, 0)
    for copy in sent:
        copy.wait_send()


def body(
    query_rows,
    key_rows,
    value_rows,
    input_gate,
    forget_gate,
    output_gate,
    documents,
    residual,
    out_weight,
    norm_gain,
    gate_weight,
    up_weight,
    down_weight,
):
    vmem = pl.BlockSpec(memory_space=pltpu.VMEM)
    hbm = pl.BlockSpec(memory_space=pl.ANY)
    dma = pltpu.SemaphoreType.DMA
    return pl.pallas_call(
        kernel,
        out_shape=pltpu.VMEM((R, D), BF),
        in_specs=[hbm] * 13,
        out_specs=vmem,
        scratch_shapes=[
            pltpu.VMEM((2, T), F32),
            pltpu.VMEM((2, T), F32),
            pltpu.VMEM((8, 128), jnp.int32),
            pltpu.VMEM((16, 128), BF),
            pltpu.VMEM((T, 256), BF),
            pltpu.VMEM((T, 256), BF),
            pltpu.VMEM((T, 256), BF),
            pltpu.VMEM((T, 256), BF),
            pltpu.VMEM((R, D), BF),
            pltpu.VMEM((64, FD), BF),
            pltpu.VMEM((64, FD), BF),
            pltpu.VMEM((64, FD), BF),
            pltpu.VMEM((TILES, 4, 4, 2, 64, 128), BF),
            pltpu.VMEM((4, 256, D), BF),
            pltpu.VMEM((264, 128), F32),
            pltpu.VMEM((264, 128), F32),
            pltpu.VMEM((256, 128), BF),
            pltpu.VMEM((8, 128), F32),
            pltpu.VMEM((LOOK, 256, 128), BF),
            pltpu.VMEM((LOOK, 8, 128), F32),
            pltpu.VMEM((4, R, 256), BF),
            pltpu.VMEM((4, R, 256), BF),
            pltpu.VMEM((1, R, 256), BF),
            pltpu.VMEM((R, D), F32),
            pltpu.VMEM((4, R, D), BF),
            pltpu.VMEM((4, R, FD), BF),
            pltpu.VMEM((3, R, D), BF),
            pltpu.VMEM((2, 128, D), BF),
            pltpu.VMEM((2, R, D), BF),
            pltpu.VMEM((128, 128), F32),
            pltpu.VMEM((128, 128), F32),
            pltpu.VMEM((16, 128), F32),
            pltpu.VMEM((8, 128), F32),
            pltpu.VMEM((16, 128), F32),
            pltpu.VMEM((2, T, 256), BF),
            pltpu.VMEM((2, T, 256), F32),
            pltpu.VMEM((T, 256), F32),
            dma((13,)),
            dma((4, 24)),
            dma((4, 24)),
            dma((9,)),
            dma((9,)),
            dma((3 * LOOK + 1,)),
            dma((3 * LOOK + 1,)),
            dma((8,)),
            dma((8,)),
            dma((8,)),
            dma((8,)),
            dma((12,)),
            dma((12,)),
        ],
        compiler_params=pltpu.CompilerParams(
            collective_id=0, has_side_effects=True, vmem_limit_bytes=62 * 1024 * 1024
        ),
    )(
        input_gate,
        forget_gate,
        documents.reshape(8, 128),
        norm_gain.reshape(16, 128),
        query_rows,
        key_rows,
        value_rows,
        output_gate,
        residual,
        out_weight,
        gate_weight,
        up_weight,
        down_weight.T,
    )


def solution(mesh):
    torus = Mesh(mesh.devices.reshape(4, 4, 2, mesh.shape["tp"]), SP_TP)
    in_specs = (
        P(SP, "tp"),
        P(SP, "tp"),
        P(SP, "tp"),
        P("tp", SP),
        P("tp", SP),
        P(SP, "tp"),
        P(SP),
        P(SP_TP, None),
        P("tp", None),
        P(),
        P(SP, "tp"),
        P(SP, "tp"),
        P("tp", SP),
    )
    out_specs = P(SP_TP, None)
    return jax.shard_map(body, mesh=torus, in_specs=in_specs, out_specs=out_specs, check_vma=False)
```

```python
import jax
import jax.numpy as jnp
from jax import lax
from jax.experimental import pallas as pl
from jax.experimental.pallas import tpu as pltpu
from jax.sharding import Mesh
from jax.sharding import PartitionSpec as P

HD = 128
SP = ("sp_0", "sp_1", "sp_2")
SP_TP = ("sp_0", "sp_1", "sp_2", "tp")
MESH = pl.DeviceIdType.MESH
BF = jnp.bfloat16
F32 = jnp.float32

NORM_EPS = 1e-06
NEG = -1e30
T = 1024
R = 256
D = 2048
FD = 1408
NJ = FD // 128
LOOK = 3
TILES = 3 * NJ
PARTS = ((0, 9, 5), (9, 13, 6), (22, 5, 3), (27, 6, 3))


def dot(a, b):
    return jnp.dot(a, b, preferred_element_type=F32)


def dot_nt(a, b):
    return lax.dot_general(a, b, (((1,), (1,)), ((), ())), preferred_element_type=F32)


def dot_tn(a, b):
    return lax.dot_general(a, b, (((0,), (0,)), ((), ())), preferred_element_type=F32)


def split(a):
    hi = a.astype(BF)
    return hi, (a - hi.astype(F32)).astype(BF)


def kernel(
    in_gate_hbm,
    forget_hbm,
    doc_hbm,
    gain_hbm,
    q_hbm,
    k_hbm,
    v_hbm,
    og_hbm,
    res_hbm,
    ow_hbm,
    wg_hbm,
    wu_hbm,
    wd_hbm,
    out,
    in_gate,
    forget,
    doc_ref,
    gain,
    q,
    k,
    v,
    og,
    res,
    wg,
    wu,
    wd,
    w,
    ow,
    st_out,
    st_twin,
    mem_out,
    meta_out,
    mem_in,
    meta_in,
    gate_out,
    gate_in,
    gate_relay,
    stream,
    rows,
    hid,
    part,
    mid,
    fin,
    vt,
    tt,
    arow,
    drow,
    gsc,
    vones,
    numden,
    opened,
    lsem,
    wss,
    wsr,
    oss,
    osr,
    sss,
    ssr,
    ass,
    asr,
    gss,
    gsr,
    rss,
    rsr,
):
    z, y, c, x = (lax.axis_index(n) for n in SP_TP)

    def step(a, by):
        return lax.rem(a + by + 8, 4)

    chip = z * 4 + y

    def chip_ahead(by):
        i = lax.rem(chip + by + 16, 16)
        return {"sp_0": i // 4, "sp_1": lax.rem(i, 4)}

    sibling = {"sp_2": 1 - c}
    peers = [sibling]
    for name, at in (("sp_0", z), ("sp_1", y), ("tp", x)):
        peers += [{name: step(at, 1)}, {name: step(at, -1)}]
    peers += [{"tp": step(x, 2)}]
    for d in range(1, LOOK + 1):
        peers += [chip_ahead(d), chip_ahead(-d)]

    barrier = pltpu.get_barrier_semaphore()
    for peer in peers:
        pl.semaphore_signal(barrier, inc=1, device_id=peer, device_id_type=MESH)

    local = []
    for n, (src, dst) in enumerate(
        (
            (in_gate_hbm, in_gate),
            (forget_hbm, forget),
            (doc_hbm, doc_ref),
            (gain_hbm, gain),
            (ow_hbm, ow.at[x]),
            (wg_hbm, wg),
            (wu_hbm, wu),
            (wd_hbm, wd),
            (k_hbm, k),
            (v_hbm, v),
            (q_hbm, q),
            (og_hbm, og),
            (res_hbm, res),
        )
    ):
        copy = pltpu.make_async_copy(src, dst, lsem.at[n])
        copy.start()
        local.append(copy)
    small, (in_ow, in_wg, in_wu, in_wd, in_k, in_v, in_q, in_og, in_res) = local[:4], local[4:]

    def remote(src, dst, send_sem, recv_sem, device):
        return pltpu.make_async_remote_copy(
            src_ref=src,
            dst_ref=dst,
            send_sem=send_sem,
            recv_sem=recv_sem,
            device_id=device,
            device_id_type=MESH,
        )

    def send(*args):
        remote(*args).start()

    def drain(ref, sem):
        remote(ref, ref, sem, lsem.at[0], sibling).wait_send()

    def arrive(ref, send_sem, recv_sem):
        remote(ref, ref, send_sem, recv_sem, sibling).wait_recv()

    def w_axes(p):
        return (("sp_0", z), ("sp_1", y)) if p % 2 == 0 else (("sp_1", y), ("sp_0", z))

    def w_at(p, first, count, uu, vv):
        zz, yy = (uu, vv) if p % 2 == 0 else (vv, uu)
        return w.at[pl.ds(first, count), zz, yy, c]

    def w_send(p, n, first, count, uu, vv, device):
        ref = w_at(p, first, count, uu, vv)
        place = (0, 1, 2, 2)[n] if n < 4 else 3 * (n // 4) + (0, 1, 2, 2)[n % 4]
        group = 2 * (n // 4 > 0) + (n % 4 > 1)
        send(ref, ref, wss.at[group], wsr.at[p, place], device)

    def w_arrive(p, place, uu, vv):
        first, count, _ = PARTS[p]
        arrive(w_at(p, first, count, uu, vv), wss.at[0], wsr.at[p, place])

    LINE = (0, -1, 1, 2)

    def w_spread(p, n):
        (_, uu), (vn, vv) = w_axes(p)
        first, count, _ = PARTS[p]
        for s, by in ((0, 1), (1, -1)):
            w_send(p, 4 + 4 * n + s, first, count, step(uu, LINE[n]), vv, {vn: step(vv, by)})

    def w_pass_on(p, n):
        (_, uu), (vn, vv) = w_axes(p)
        first, count, half = PARTS[p]
        k_at = step(uu, LINE[n])
        w_arrive(p, 3 + 3 * n, k_at, step(vv, -1))
        w_send(p, 6 + 4 * n, first, half, k_at, step(vv, -1), {vn: step(vv, 1)})
        w_arrive(p, 4 + 3 * n, k_at, step(vv, 1))
        w_send(p, 7 + 4 * n, first + half, count - half, k_at, step(vv, 1), {vn: step(vv, -1)})

    def w_line(p, n):
        (_, uu), _ = w_axes(p)
        first, count, _ = PARTS[p]
        k_at = step(uu, LINE[n])
        span = pl.ds(first, count)
        ref = w.at[span, k_at, :, c] if p % 2 == 0 else w.at[span, :, k_at, c]
        send(ref, ref, wss.at[4 + p // 2], wsr.at[0, 15 + p // 2], sibling)

    def w_twin(kind):
        first, count = ((0, 2 * NJ), (2 * NJ, NJ))[kind]
        arrive(w.at[pl.ds(first, count), :, :, 1 - c], wss.at[0], wsr.at[0, 15 + kind])

    def w_finish(p, n):
        (_, uu), (_, vv) = w_axes(p)
        w_arrive(p, 5 + 3 * n, step(uu, LINE[n]), step(vv, 2))
        w_line(p, n)

    def w_0(name):
        for p in (0, 1, 2, 3) if name == "sp_0" else (1, 0, 3, 2):
            (un, uu), (_, vv) = w_axes(p)
            first, count, _ = PARTS[p]
            if un == name:
                for n, by in ((0, 1), (1, -1)):
                    w_send(p, n, first, count, uu, vv, {un: step(uu, by)})
            else:
                w_spread(p, 0)

    def w_1(p):
        (un, uu), (_, vv) = w_axes(p)
        first, count, half = PARTS[p]
        w_arrive(p, 0, step(uu, -1), vv)
        w_send(p, 2, first, half, step(uu, -1), vv, {un: step(uu, 1)})
        w_spread(p, 1)
        w_arrive(p, 1, step(uu, 1), vv)
        w_send(p, 3, first + half, count - half, step(uu, 1), vv, {un: step(uu, -1)})
        w_spread(p, 2)

    def w_2(p):
        (_, uu), (_, vv) = w_axes(p)
        w_arrive(p, 2, step(uu, 2), vv)
        w_spread(p, 3)

    right, left, across = {"tp": step(x, 1)}, {"tp": step(x, -1)}, {"tp": step(x, 2)}
    x_r, x_l, x_a = step(x, 1), step(x, -1), step(x, 2)

    def o_at(slot, part_first, count):
        return ow.at[slot, pl.ds(c * 128 + part_first, count)]

    def o_send(n, slot, first, count, device):
        send(o_at(slot, first, count), o_at(slot, first, count), oss, osr.at[n], device)


    def o_arrive(n, slot, first, count):
        arrive(o_at(slot, first, count), oss, osr.at[n])

    pl.semaphore_wait(barrier, len(peers))
    in_ow.wait()
    o_send(0, x, 0, 64, right)
    o_send(1, x, 64, 64, left)
    o_send(2, x, 64, 64, right)
    o_send(2, x, 0, 64, left)

    in_wg.wait()
    in_wu.wait()
    in_wd.wait()
    for j in range(NJ):
        cols = slice(128 * j, 128 * j + 128)
        w[2 * j, z, y, c] = wg[:, cols]
        w[2 * j + 1, z, y, c] = wu[:, cols]
        w[2 * NJ + j, z, y, c] = wd[:, cols]

    w_0("sp_0")

    for copy in small:
        copy.wait()
    lane = lax.broadcasted_iota(jnp.int32, (8, 128), 1)
    row = lax.broadcasted_iota(jnp.int32, (8, 128), 0)
    docs = doc_ref[...].astype(F32)
    drow[...] = docs
    gsc[...] = gain[...].astype(F32)
    last_lane = jnp.broadcast_to(docs[:, 127:128], (8, 128))
    heads = []
    vt[...] = jnp.zeros_like(vt)

    def eight_rows(ref, h):
        return jnp.concatenate([ref[h : h + 1, 128 * n : 128 * n + 128] for n in range(8)], axis=0)

    for h in range(2):
        cum = eight_rows(forget, h)
        cum = jnp.minimum(cum, 0.0) - jnp.log1p(jnp.exp(-jnp.abs(cum)))
        for s in (1, 2, 4, 8, 16, 32, 64):
            cum = cum + jnp.where(lane >= s, pltpu.roll(cum, s, 1), 0.0)
        upto = jnp.broadcast_to(cum[:, 127:128], (8, 128))
        for s in (1, 2, 4):
            upto = upto + jnp.where(row >= s, pltpu.roll(upto, s, 0), 0.0)
        cum = cum + jnp.where(row >= 1, pltpu.roll(upto, 1, 0), 0.0)
        a = eight_rows(in_gate, h) - cum
        m = a
        for s in (1, 2, 4, 8, 16, 32, 64):
            ok = (lane >= s) & (pltpu.roll(docs, s, 1) == docs)
            m = jnp.where(ok, jnp.maximum(m, pltpu.roll(m, s, 1)), m)
        e = jnp.broadcast_to(m[:, 127:128], (8, 128))
        for s in (1, 2, 4):
            ok = (row >= s) & (pltpu.roll(last_lane, s, 0) == last_lane)
            e = jnp.where(ok, jnp.maximum(e, pltpu.roll(e, s, 0)), e)
        ok = (row >= 1) & (pltpu.roll(last_lane, 1, 0) == docs)
        m = jnp.where(ok, jnp.maximum(m, pltpu.roll(e, 1, 0)), m)
        top = e[7:8, :]
        last = last_lane[7:8, :]
        weight = jnp.where(docs == last, jnp.exp(a - top), 0.0)
        arow[8 * h : 8 * h + 8, :] = a
        vt[8 * h : 8 * h + 8, :] = m
        vt[16 + 8 * h : 24 + 8 * h, :] = weight
        total = upto[7:8, :]
        heads.append((top + total, total, m))
    vt[32:40, :] = docs
    tt[...] = vt[...].T

    in_k.wait()
    in_v.wait()
    normers = []
    for h in range(2):
        cols = slice(h * HD, h * HD + HD)
        kw = jnp.concatenate(
            [
                k[128 * n : 128 * n + 128, cols].astype(F32)
                * tt[:, 16 + 8 * h + n : 17 + 8 * h + n]
                for n in range(8)
            ],
            axis=0,
        )
        hi, lo = split(kw)
        st_out[HD * h : HD * h + HD, :] = dot_tn(hi, v[:, cols]) + dot_tn(lo, v[:, cols])
        normers.append(jnp.sum(kw, axis=0, keepdims=True))
    st_out[256:264, :] = jnp.concatenate(
        normers
        + [heads[0][0], heads[1][0], heads[0][1], heads[1][1], last, last],
        axis=0,
    )

    send(st_out, st_twin, sss.at[0], ssr.at[0], sibling)

    arrive(st_twin, sss.at[0], ssr.at[0])
    first_core = c == 0
    mine, twin = st_out[256:264, :], st_twin[256:264, :]
    early = jnp.where(first_core, mine, twin)
    late = jnp.where(first_core, twin, mine)
    goes = early[6:7, :] == late[6:7, :]
    meta = [None] * 8
    for h in range(2):
        span = slice(HD * h, HD * h + HD)
        one = jnp.where(goes, early[2 + h : 3 + h, :] + late[4 + h : 5 + h, :], NEG)
        two = late[2 + h : 3 + h, :]
        stab = jnp.maximum(one, two)
        share_one = jnp.where(goes, jnp.exp(one - stab), 0.0)
        share_two = jnp.exp(two - stab)
        share_mine = jnp.where(first_core, share_one, share_two)
        share_twin = jnp.where(first_core, share_two, share_one)
        mem_out[span, :] = (share_mine * st_out[span, :] + share_twin * st_twin[span, :]).astype(BF)
        meta[h] = share_mine * mine[h : h + 1, :] + share_twin * twin[h : h + 1, :]
        meta[2 + h] = stab
        meta[4 + h] = early[4 + h : 5 + h, :] + late[4 + h : 5 + h, :]
    meta[6] = meta[7] = late[6:7, :]
    meta_out[...] = jnp.concatenate(meta, axis=0)
    head = pl.ds(HD * c, HD)
    for d in range(1, LOOK + 1):
        send(meta_out, meta_in.at[d - 1], sss.at[1], ssr.at[1], chip_ahead(d))
        send(mem_out.at[head], mem_in.at[d - 1, head], sss.at[2], ssr.at[2], chip_ahead(d))

    w_0("sp_1")

    in_q.wait()
    for h in range(2):
        vones[h, :, :HD] = v[:, HD * h : HD * h + HD]
        vones[h, :, HD:] = jnp.ones((T, HD), BF)

    def column(n):
        return jnp.concatenate([tt[:, n : n + 1], tt[:, n + 1 : n + 2]], axis=0)

    for h in range(2):
        cols = slice(h * HD, h * HD + HD)
        for i in range(4):
            at = slice(256 * i, 256 * i + 256)
            m_col, d_col = column(8 * h + 2 * i), column(32 + 2 * i)
            acc = jnp.zeros((256, 2 * HD), F32)
            for j in range(i + 1):
                keys = slice(256 * j, 256 * j + 256)
                a_row, d_row = (
                    jnp.concatenate([ref[n + 2 * j : n + 2 * j + 1, :], ref[n + 2 * j + 1 : n + 2 * j + 2, :]], axis=1)
                    for ref, n in ((arow, 8 * h), (drow, 0))
                )
                ok = d_col == d_row
                if i == j:
                    ok = ok & (
                        lax.broadcasted_iota(jnp.int32, (256, 256), 0)
                        >= lax.broadcasted_iota(jnp.int32, (256, 256), 1)
                    )
                p = jnp.where(ok, dot_nt(q[at, cols], k[keys, cols]) * jnp.exp(a_row - m_col), 0.0)
                hi, lo = split(p)
                acc = acc + (dot(hi, vones[h, keys, :]) + dot(lo, vones[h, keys, :]))
            numden[h, at, :] = acc
    in_og.wait()
    for i in range(4):
        at = slice(256 * i, 256 * i + 256)
        opened[at, :] = 1.0 / (1.0 + jnp.exp(-og[at, :].astype(F32)))

    o_arrive(0, x_l, 0, 64)
    o_send(3, x_l, 0, 64, right)
    o_arrive(1, x_r, 64, 64)
    o_send(3, x_r, 64, 64, left)
    arrive(mem_in.at[:, head], sss.at[2], ssr.at[2])
    for d in range(LOOK):
        send(mem_in.at[d, head], mem_in.at[d, head], sss.at[2], ssr.at[3], sibling)
    arrive(meta_in, sss.at[1], ssr.at[1])
    arrive(mem_in.at[:, pl.ds(HD * (1 - c), HD)], sss.at[2], ssr.at[3])
    second_core = c == 1
    one_back = meta_in[0, 6:7, :]
    carry_doc = jnp.where(second_core, twin[6:7, :], jnp.where(chip > 0, one_back, -1.0))
    scale = HD**-0.5
    memories = []
    for h in range(2):
        passed = jnp.where(second_core, twin[4 + h : 5 + h, :], 0.0)
        levels = [jnp.where(second_core, twin[2 + h : 3 + h, :], NEG)]
        for d in range(1, LOOK + 1):
            ok = (meta_in[d - 1, 6:7, :] == carry_doc) & (chip >= d)
            levels.append(jnp.where(ok, meta_in[d - 1, 2 + h : 3 + h, :] + passed, NEG))
            passed = passed + meta_in[d - 1, 4 + h : 5 + h, :]
        stab = levels[0]
        for level in levels[1:]:
            stab = jnp.maximum(stab, level)
        shares = [jnp.where(level > 0.5 * NEG, jnp.exp(level - stab), 0.0) for level in levels]
        memory = shares[0] * st_twin[HD * h : HD * h + HD, :]
        normer = shares[0] * twin[h : h + 1, :]
        for d in range(1, LOOK + 1):
            memory = memory + shares[d] * mem_in[d - 1, HD * h : HD * h + HD, :].astype(F32)
            normer = normer + shares[d] * meta_in[d - 1, h : h + 1, :]
        memories.append(memory)
        m = heads[h][2]
        goes_on = docs == carry_doc
        both = jnp.where(goes_on, jnp.maximum(m, stab), m)
        vt[8 * h : 8 * h + 8, :] = jnp.exp(m - both) * scale
        vt[16 + 8 * h : 24 + 8 * h, :] = jnp.where(goes_on, jnp.exp(stab - both), 0.0) * scale
        vt[32 + 8 * h : 40 + 8 * h, :] = jnp.broadcast_to(normer, (8, HD))
    tt[...] = vt[...].T
    for h in range(2):
        cols = slice(h * HD, h * HD + HD)
        normer = jnp.broadcast_to(tt[:, 32 + 8 * h : 33 + 8 * h], (HD, HD))
        parts = [jnp.concatenate(pair, axis=1) for pair in zip(split(memories[h]), split(normer))]
        for i in range(4):
            at = slice(256 * i, 256 * i + 256)
            scale_in, scale_by = column(8 * h + 2 * i), column(16 + 8 * h + 2 * i)
            queries = q[at, cols]
            both = scale_in * numden[h, at, :] + scale_by * (dot(queries, parts[0]) + dot(queries, parts[1]))
            cell = both[:, :HD] / jnp.maximum(jnp.abs(both[:, HD:]), 1.0)
            gate_out[i, :, cols] = (cell * opened[at, cols]).astype(BF)

    def half_of(ref, slot, half):
        return ref.at[slot, pl.ds(128 * half, 128)]

    onward, behind = {"tp": lax.rem(x + 1 + 2 * c, 4)}, lax.rem(x + 3 + 2 * c, 4)

    def g_send(n, half, src, dst, device):
        send(half_of(*src, half), half_of(*dst, half), ass, asr.at[2 * n + half], device)

    for half in range(2):
        g_send(0, half, (gate_out, x_a), (gate_relay, 0), onward)
    for half in range(2):
        g_send(1, half, (gate_out, x_r), (gate_in, x), right)
        g_send(1, half, (gate_out, x_l), (gate_in, x), left)

    def relay(half):
        arrive(half_of(gate_relay, 0, half), ass, asr.at[half])
        g_send(1, half, (gate_relay, 0), (gate_in, behind), onward)

    gate_in[x] = gate_out[x]

    w_1(0)
    w_pass_on(1, 0)
    w_1(1)
    w_pass_on(0, 0)
    o_arrive(2, x_l, 0, 128)
    for slot in (x_l, x_r):
        o_send(4, slot, 0, 128, sibling)
    w_1(2)
    w_pass_on(3, 0)
    w_1(3)
    w_pass_on(2, 0)
    o_arrive(3, x_a, 0, 128)
    o_send(4, x_a, 0, 128, sibling)
    relay(0)
    relay(1)
    arrive(ow.at[pl.ds(0, 3), pl.ds((1 - c) * 128, 128)], oss, osr.at[4])
    in_res.wait()

    def output_rows(half):
        span = pl.ds(128 * half, 128)

        def project(n, squares):
            cols = pl.ds(pl.multiple_of(n * 256, 256), 256)
            cells = jnp.concatenate([gate_in[n, span] for n in range(4)], axis=1)
            acc = res[span, cols].astype(F32) + dot(cells, ow[:, :, cols].reshape(1024, 256))
            stream[span, cols] = acc
            return squares + (acc[:, :128] * acc[:, :128] + acc[:, 128:] * acc[:, 128:])

        squares = lax.fori_loop(0, D // 256, project, jnp.zeros((128, 128), F32))
        inverse = lax.rsqrt(jnp.sum(squares, axis=1, keepdims=True) / D + NORM_EPS)

        def normalize(n, carry):
            cols = pl.ds(pl.multiple_of(n * 256, 256), 256)
            gain_row = jnp.concatenate([gsc[pl.ds(2 * n, 1), :], gsc[pl.ds(2 * n + 1, 1), :]], axis=1)
            rows[x, span, cols] = (stream[span, cols] * inverse * gain_row).astype(BF)
            return carry

        lax.fori_loop(0, D // 256, normalize, 0)

    def r_at(slot, first, count):
        return rows.at[slot, pl.ds(first, count)]

    def r_send(n, slot, first, count, device):
        send(r_at(slot, first, count), r_at(slot, first, count), gss, gsr.at[n], device)

    def r_arrive(n, slot, first, count):
        arrive(r_at(slot, first, count), gss, gsr.at[n])

    def gated_rows(half):
        arrive(gate_in.at[pl.ds(0, 3), pl.ds(128 * half, 128)], ass, asr.at[2 + half])

    gated_rows(0)
    output_rows(0)
    r_send(0, x, 0, 128, right)
    r_send(1, x, 0, 128, left)
    gated_rows(1)
    output_rows(1)
    r_send(1, x, 128, 128, right)
    r_send(2, x, 128, 64, left)
    r_send(3, x, 192, 64, left)

    w_2(0)
    w_2(1)
    for n in (1, 2):
        w_pass_on(0, n)
        w_pass_on(1, n)
    w_finish(0, 0)
    w_finish(1, 0)
    w_2(2)
    w_2(3)
    w_pass_on(1, 3)
    w_pass_on(0, 3)
    for n in (1, 2):
        w_pass_on(2, n)
        w_pass_on(3, n)
    r_arrive(0, x_l, 0, 128)
    r_send(4, x_l, 0, 128, right)
    for n in (1, 2):
        w_finish(0, n)
        w_finish(1, n)
    w_pass_on(3, 3)
    w_pass_on(2, 3)
    w_finish(0, 3)
    w_finish(1, 3)
    for n in (0, 1, 2):
        w_finish(2, n)
        w_finish(3, n)
    r_arrive(2, x_r, 128, 64)
    r_send(4, x_r, 128, 64, left)
    r_arrive(3, x_r, 192, 64)
    r_send(4, x_r, 192, 64, left)
    w_finish(2, 3)
    w_finish(3, 3)
    w_twin(0)

    up_half, low_half = pl.ds(0, 128), pl.ds(128, 128)

    def widen(n, pieces):
        def one(j, carry):
            both = jnp.concatenate(
                [w[2 * j].reshape(D, 128), w[2 * j + 1].reshape(D, 128)], axis=1
            )
            acts = dot(jnp.concatenate([rows[piece] for piece in pieces], axis=0), both)
            gate_act, up_act = acts[:, :128], acts[:, 128:]
            cols = pl.ds(pl.multiple_of(j * 128, 128), 128)
            hid[n, :, cols] = (gate_act * (1.0 / (1.0 + jnp.exp(-gate_act))) * up_act).astype(BF)
            return carry

        lax.fori_loop(0, NJ, one, 0)

    def narrow(n, store, first=0, last=D // 256):
        def one(t, carry):
            down = jnp.concatenate(
                [
                    w[2 * NJ + j, t // 2, pl.ds(2 * lax.rem(t, 2), 2)].reshape(256, 128)
                    for j in range(NJ)
                ],
                axis=1,
            )
            store(pl.ds(pl.multiple_of(t * 256, 256), 256), dot_nt(hid[n], down))
            return carry

        lax.fori_loop(first, last, one, 0)

    def keep(n):
        def store(cols, value):
            part[n, :, cols] = value.astype(BF)

        return store

    def p_send(n, src, dst, device):
        send(src, dst, rss, rsr.at[n], device)

    def p_arrive(n, ref):
        arrive(ref, rss, rsr.at[n])

    def piece(ref, slot, half, side):
        return ref.at[slot, half, pl.ds(1024 * side, 1024)]

    widen(0, ((x_l, up_half), (x_r, low_half)))
    w_twin(1)
    for side in range(2):
        narrow(0, keep(0), 4 * side, 4 * side + 4)
        p_send(side, piece(part, 0, low_half, side), piece(fin, 0, low_half, side), right)
        p_send(side, piece(part, 0, up_half, side), piece(fin, 1, up_half, side), left)
    r_arrive(4, x_a, 0, R)
    widen(2, ((x_a, up_half), (x_a, low_half)))
    for side in range(2):
        narrow(2, keep(2), 4 * side, 4 * side + 4)
        p_send(2 + side, piece(part, 2, up_half, side), piece(mid, 0, up_half, side), right)
        p_send(2 + side, piece(part, 2, low_half, side), piece(mid, 1, up_half, side), left)
    r_arrive(1, x_r, 0, R)
    widen(1, ((x_r, up_half), (x_l, low_half)))
    narrow(1, keep(1))

    def pass_sum(side):
        at = pl.ds(1024 * side, 1024)
        p_arrive(2 + side, mid.at[:, :, at])
        part[1, up_half, at] = (part[1, up_half, at].astype(F32) + mid[0, :, at].astype(F32)).astype(BF)
        p_send(side, piece(part, 1, up_half, side), piece(fin, 0, up_half, side), right)
        part[1, low_half, at] = (part[1, low_half, at].astype(F32) + mid[1, :, at].astype(F32)).astype(BF)
        p_send(side, piece(part, 1, low_half, side), piece(fin, 1, low_half, side), left)

    pass_sum(0)
    widen(3, ((x, up_half), (x, low_half)))
    pass_sum(1)
    def own(cols, value):
        stream[:, cols] = stream[:, cols] + 0.5 * value

    narrow(3, own)
    for side in range(2):
        at = pl.ds(1024 * side, 1024)
        p_arrive(side, fin.at[:, :, at])

        def finish(n, carry):
            cols = pl.ds(pl.multiple_of(n * 256, 256), 256)
            others = fin[0, :, cols].astype(F32) + fin[1, :, cols].astype(F32)
            out[:, cols] = (stream[:, cols] + 0.5 * others).astype(BF)
            return carry

        lax.fori_loop(4 * side, 4 * side + 4, finish, 0)

    drain(w.at[:, pl.ds(0, 1), pl.ds(0, 1)], wss.at[0])
    drain(w.at[:, pl.ds(0, 1), pl.ds(0, 1), pl.ds(0, 1)], wss.at[1])
    drain(w.at[:, pl.ds(0, 1)], wss.at[2])
    drain(w.at[:, pl.ds(0, 1), :, pl.ds(0, 1)], wss.at[3])
    drain(w.at[pl.ds(0, 2 * NJ), :, :, pl.ds(0, 1)], wss.at[4])
    drain(w.at[pl.ds(0, NJ), :, :, pl.ds(0, 1)], wss.at[5])
    drain(ow.at[pl.ds(0, 3)], oss)
    drain(st_out, sss.at[0])
    drain(meta_in, sss.at[1])
    drain(mem_in, sss.at[2])
    drain(gate_in, ass)
    drain(rows.at[pl.ds(0, 3)], gss)
    drain(part, rss)


def body(
    query_rows,
    key_rows,
    value_rows,
    input_gate,
    forget_gate,
    output_gate,
    documents,
    residual,
    out_weight,
    norm_gain,
    gate_weight,
    up_weight,
    down_weight,
):
    vmem = pl.BlockSpec(memory_space=pltpu.VMEM)
    hbm = pl.BlockSpec(memory_space=pl.ANY)
    dma = pltpu.SemaphoreType.DMA
    return pl.pallas_call(
        kernel,
        out_shape=pltpu.VMEM((R, D), BF),
        in_specs=[hbm] * 13,
        out_specs=vmem,
        scratch_shapes=[
            pltpu.VMEM((2, T), F32),
            pltpu.VMEM((2, T), F32),
            pltpu.VMEM((8, 128), jnp.int32),
            pltpu.VMEM((16, 128), BF),
            pltpu.VMEM((T, 256), BF),
            pltpu.VMEM((T, 256), BF),
            pltpu.VMEM((T, 256), BF),
            pltpu.VMEM((T, 256), BF),
            pltpu.VMEM((R, D), BF),
            pltpu.VMEM((64, FD), BF),
            pltpu.VMEM((64, FD), BF),
            pltpu.VMEM((64, FD), BF),
            pltpu.VMEM((TILES, 4, 4, 2, 64, 128), BF),
            pltpu.VMEM((4, 256, D), BF),
            pltpu.VMEM((264, 128), F32),
            pltpu.VMEM((264, 128), F32),
            pltpu.VMEM((256, 128), BF),
            pltpu.VMEM((8, 128), F32),
            pltpu.VMEM((LOOK, 256, 128), BF),
            pltpu.VMEM((LOOK, 8, 128), F32),
            pltpu.VMEM((4, R, 256), BF),
            pltpu.VMEM((4, R, 256), BF),
            pltpu.VMEM((1, R, 256), BF),
            pltpu.VMEM((R, D), F32),
            pltpu.VMEM((4, R, D), BF),
            pltpu.VMEM((4, R, FD), BF),
            pltpu.VMEM((3, R, D), BF),
            pltpu.VMEM((2, 128, D), BF),
            pltpu.VMEM((2, R, D), BF),
            pltpu.VMEM((128, 128), F32),
            pltpu.VMEM((128, 128), F32),
            pltpu.VMEM((16, 128), F32),
            pltpu.VMEM((8, 128), F32),
            pltpu.VMEM((16, 128), F32),
            pltpu.VMEM((2, T, 256), BF),
            pltpu.VMEM((2, T, 256), F32),
            pltpu.VMEM((T, 256), F32),
            dma((13,)),
            dma((6,)),
            dma((4, 17)),
            dma(()),
            dma((5,)),
            dma((3,)),
            dma((4,)),
            dma(()),
            dma((4,)),
            dma(()),
            dma((5,)),
            dma(()),
            dma((4,)),
        ],
        compiler_params=pltpu.CompilerParams(
            collective_id=0, has_side_effects=True, vmem_limit_bytes=62 * 1024 * 1024
        ),
    )(
        input_gate,
        forget_gate,
        documents.reshape(8, 128),
        norm_gain.reshape(16, 128),
        query_rows,
        key_rows,
        value_rows,
        output_gate,
        residual,
        out_weight,
        gate_weight,
        up_weight,
        down_weight.T,
    )


def solution(mesh):
    torus = Mesh(mesh.devices.reshape(4, 4, 2, mesh.shape["tp"]), SP_TP)
    in_specs = (
        P(SP, "tp"),
        P(SP, "tp"),
        P(SP, "tp"),
        P("tp", SP),
        P("tp", SP),
        P(SP, "tp"),
        P(SP),
        P(SP_TP, None),
        P("tp", None),
        P(),
        P(SP, "tp"),
        P(SP, "tp"),
        P("tp", SP),
    )
    out_specs = P(SP_TP, None)
    return jax.shard_map(body, mesh=torus, in_specs=in_specs, out_specs=out_specs, check_vma=False)
```

```python
import jax
import jax.numpy as jnp
from jax import lax
from jax.experimental import pallas as pl
from jax.experimental.pallas import tpu as pltpu
from jax.sharding import Mesh
from jax.sharding import PartitionSpec as P

HD = 128
SP = ("sp_0", "sp_1", "sp_2")
SP_TP = ("sp_0", "sp_1", "sp_2", "tp")
MESH = pl.DeviceIdType.MESH
BF = jnp.bfloat16
F32 = jnp.float32

NORM_EPS = 1e-06
NEG = -1e30
T = 1024
R = 256
D = 2048
FD = 1408
NJ = FD // 128
LOOK = 3
TILES = 3 * NJ
PARTS = ((0, 9, 5), (9, 13, 6), (22, 5, 3), (27, 6, 3))


def dot(a, b):
    return jnp.dot(a, b, preferred_element_type=F32)


def dot_nt(a, b):
    return lax.dot_general(a, b, (((1,), (1,)), ((), ())), preferred_element_type=F32)


def dot_tn(a, b):
    return lax.dot_general(a, b, (((0,), (0,)), ((), ())), preferred_element_type=F32)


def split(a):
    hi = a.astype(BF)
    return hi, (a - hi.astype(F32)).astype(BF)


def kernel(
    in_gate_hbm,
    forget_hbm,
    doc_hbm,
    gain_hbm,
    q_hbm,
    k_hbm,
    v_hbm,
    og_hbm,
    res_hbm,
    ow_hbm,
    wg_hbm,
    wu_hbm,
    wd_hbm,
    out,
    in_gate,
    forget,
    doc_ref,
    gain,
    q,
    k,
    v,
    og,
    res,
    wg,
    wu,
    wd,
    w,
    ow,
    st_out,
    st_twin,
    mem_out,
    meta_out,
    mem_in,
    meta_in,
    gate_out,
    gate_in,
    gate_relay,
    stream,
    rows,
    hid,
    part,
    mid,
    fin,
    vt,
    tt,
    arow,
    drow,
    gsc,
    vones,
    numden,
    opened,
    inverses,
    factor,
    lsem,
    wss,
    wsr,
    oss,
    osr,
    sss,
    ssr,
    ass,
    asr,
    gss,
    gsr,
    iss,
    isr,
    rss,
    rsr,
):
    z, y, c, x = (lax.axis_index(n) for n in SP_TP)

    def step(a, by):
        return lax.rem(a + by + 8, 4)

    chip = z * 4 + y

    def chip_ahead(by):
        i = lax.rem(chip + by + 16, 16)
        return {"sp_0": i // 4, "sp_1": lax.rem(i, 4)}

    sibling = {"sp_2": 1 - c}
    peers = [sibling]
    for name, at in (("sp_0", z), ("sp_1", y), ("tp", x)):
        peers += [{name: step(at, 1)}, {name: step(at, -1)}]
    peers += [{"tp": step(x, 2)}]
    for d in range(1, LOOK + 1):
        peers += [chip_ahead(d), chip_ahead(-d)]

    barrier = pltpu.get_barrier_semaphore()
    for peer in peers:
        pl.semaphore_signal(barrier, inc=1, device_id=peer, device_id_type=MESH)

    local = []
    for n, (src, dst) in enumerate(
        (
            (in_gate_hbm, in_gate),
            (forget_hbm, forget),
            (doc_hbm, doc_ref),
            (gain_hbm, gain),
            (ow_hbm, ow.at[x]),
            (wg_hbm, wg),
            (wu_hbm, wu),
            (wd_hbm, wd),
            (k_hbm, k),
            (v_hbm, v),
            (q_hbm, q),
            (og_hbm, og),
            (res_hbm, res),
        )
    ):
        copy = pltpu.make_async_copy(src, dst, lsem.at[n])
        copy.start()
        local.append(copy)
    small, (in_ow, in_wg, in_wu, in_wd, in_k, in_v, in_q, in_og, in_res) = local[:4], local[4:]

    def remote(src, dst, send_sem, recv_sem, device):
        return pltpu.make_async_remote_copy(
            src_ref=src,
            dst_ref=dst,
            send_sem=send_sem,
            recv_sem=recv_sem,
            device_id=device,
            device_id_type=MESH,
        )

    def send(*args):
        remote(*args).start()

    def drain(ref, sem):
        remote(ref, ref, sem, lsem.at[0], sibling).wait_send()

    def arrive(ref, send_sem, recv_sem):
        remote(ref, ref, send_sem, recv_sem, sibling).wait_recv()

    def w_axes(p):
        return (("sp_0", z), ("sp_1", y)) if p % 2 == 0 else (("sp_1", y), ("sp_0", z))

    def w_at(p, first, count, uu, vv):
        zz, yy = (uu, vv) if p % 2 == 0 else (vv, uu)
        return w.at[pl.ds(first, count), zz, yy, c]

    def w_send(p, n, first, count, uu, vv, device):
        ref = w_at(p, first, count, uu, vv)
        place = (0, 1, 2, 2)[n] if n < 4 else 3 * (n // 4) + (0, 1, 2, 2)[n % 4]
        group = 2 * (n // 4 > 0) + (n % 4 > 1)
        send(ref, ref, wss.at[group], wsr.at[p, place], device)

    def w_arrive(p, place, uu, vv):
        first, count, _ = PARTS[p]
        arrive(w_at(p, first, count, uu, vv), wss.at[0], wsr.at[p, place])

    LINE = (0, -1, 1, 2)

    def w_spread(p, n):
        (_, uu), (vn, vv) = w_axes(p)
        first, count, _ = PARTS[p]
        for s, by in ((0, 1), (1, -1)):
            w_send(p, 4 + 4 * n + s, first, count, step(uu, LINE[n]), vv, {vn: step(vv, by)})

    def w_pass_on(p, n):
        (_, uu), (vn, vv) = w_axes(p)
        first, count, half = PARTS[p]
        k_at = step(uu, LINE[n])
        w_arrive(p, 3 + 3 * n, k_at, step(vv, -1))
        w_send(p, 6 + 4 * n, first, half, k_at, step(vv, -1), {vn: step(vv, 1)})
        w_arrive(p, 4 + 3 * n, k_at, step(vv, 1))
        w_send(p, 7 + 4 * n, first + half, count - half, k_at, step(vv, 1), {vn: step(vv, -1)})
        for by in (0, -1, 1) if p < 2 else ():
            w_hand_over(p, n, by)

    def w_hand_over(p, n, by):
        (_, uu), (_, vv) = w_axes(p)
        first, count, _ = PARTS[p]
        ref = w_at(p, first, count, step(uu, LINE[n]), step(vv, by))
        send(ref, ref, wss.at[4 + p // 2], wsr.at[0, 15 + p // 2], sibling)

    def w_twin(kind):
        first, count = ((0, 2 * NJ), (2 * NJ, NJ))[kind]
        arrive(w.at[pl.ds(first, count), :, :, 1 - c], wss.at[0], wsr.at[0, 15 + kind])

    def w_finish(p, n):
        (_, uu), (_, vv) = w_axes(p)
        w_arrive(p, 5 + 3 * n, step(uu, LINE[n]), step(vv, 2))
        for by in (2,) if p < 2 else (0, -1, 1, 2):
            w_hand_over(p, n, by)

    def w_0(name):
        for p in (0, 1, 2, 3) if name == "sp_0" else (1, 0, 3, 2):
            (un, uu), (_, vv) = w_axes(p)
            first, count, _ = PARTS[p]
            if un == name:
                for n, by in ((0, 1), (1, -1)):
                    w_send(p, n, first, count, uu, vv, {un: step(uu, by)})
            else:
                w_spread(p, 0)

    def w_1(p):
        (un, uu), (_, vv) = w_axes(p)
        first, count, half = PARTS[p]
        w_arrive(p, 0, step(uu, -1), vv)
        w_send(p, 2, first, half, step(uu, -1), vv, {un: step(uu, 1)})
        w_spread(p, 1)
        w_arrive(p, 1, step(uu, 1), vv)
        w_send(p, 3, first + half, count - half, step(uu, 1), vv, {un: step(uu, -1)})
        w_spread(p, 2)

    def w_2(p):
        (_, uu), (_, vv) = w_axes(p)
        w_arrive(p, 2, step(uu, 2), vv)
        w_spread(p, 3)

    right, left, across = {"tp": step(x, 1)}, {"tp": step(x, -1)}, {"tp": step(x, 2)}
    x_r, x_l, x_a = step(x, 1), step(x, -1), step(x, 2)

    def o_at(slot, part_first, count):
        return ow.at[slot, pl.ds(c * 128 + part_first, count)]

    def o_send(n, slot, first, count, device):
        send(o_at(slot, first, count), o_at(slot, first, count), oss, osr.at[n], device)


    def o_arrive(n, slot, first, count):
        arrive(o_at(slot, first, count), oss, osr.at[n])

    pl.semaphore_wait(barrier, len(peers))
    in_ow.wait()
    o_send(0, x, 0, 64, right)
    o_send(1, x, 64, 64, left)
    o_send(2, x, 64, 64, right)
    o_send(2, x, 0, 64, left)

    in_wg.wait()
    in_wu.wait()
    in_wd.wait()
    for j in range(NJ):
        cols = slice(128 * j, 128 * j + 128)
        w[2 * j, z, y, c] = wg[:, cols]
        w[2 * j + 1, z, y, c] = wu[:, cols]
        w[2 * NJ + j, z, y, c] = wd[:, cols]

    w_0("sp_0")

    for copy in small:
        copy.wait()
    lane = lax.broadcasted_iota(jnp.int32, (8, 128), 1)
    row = lax.broadcasted_iota(jnp.int32, (8, 128), 0)
    docs = doc_ref[...].astype(F32)
    drow[...] = docs
    gsc[...] = gain[...].astype(F32)
    last_lane = jnp.broadcast_to(docs[:, 127:128], (8, 128))
    heads = []
    vt[...] = jnp.zeros_like(vt)

    def eight_rows(ref, h):
        return jnp.concatenate([ref[h : h + 1, 128 * n : 128 * n + 128] for n in range(8)], axis=0)

    for h in range(2):
        cum = eight_rows(forget, h)
        cum = jnp.minimum(cum, 0.0) - jnp.log1p(jnp.exp(-jnp.abs(cum)))
        for s in (1, 2, 4, 8, 16, 32, 64):
            cum = cum + jnp.where(lane >= s, pltpu.roll(cum, s, 1), 0.0)
        upto = jnp.broadcast_to(cum[:, 127:128], (8, 128))
        for s in (1, 2, 4):
            upto = upto + jnp.where(row >= s, pltpu.roll(upto, s, 0), 0.0)
        cum = cum + jnp.where(row >= 1, pltpu.roll(upto, 1, 0), 0.0)
        a = eight_rows(in_gate, h) - cum
        m = a
        for s in (1, 2, 4, 8, 16, 32, 64):
            ok = (lane >= s) & (pltpu.roll(docs, s, 1) == docs)
            m = jnp.where(ok, jnp.maximum(m, pltpu.roll(m, s, 1)), m)
        e = jnp.broadcast_to(m[:, 127:128], (8, 128))
        for s in (1, 2, 4):
            ok = (row >= s) & (pltpu.roll(last_lane, s, 0) == last_lane)
            e = jnp.where(ok, jnp.maximum(e, pltpu.roll(e, s, 0)), e)
        ok = (row >= 1) & (pltpu.roll(last_lane, 1, 0) == docs)
        m = jnp.where(ok, jnp.maximum(m, pltpu.roll(e, 1, 0)), m)
        top = e[7:8, :]
        last = last_lane[7:8, :]
        weight = jnp.where(docs == last, jnp.exp(a - top), 0.0)
        arow[8 * h : 8 * h + 8, :] = a
        vt[8 * h : 8 * h + 8, :] = m
        vt[16 + 8 * h : 24 + 8 * h, :] = weight
        total = upto[7:8, :]
        heads.append((top + total, total, m))
    vt[32:40, :] = docs
    tt[...] = vt[...].T

    in_k.wait()
    in_v.wait()
    normers = []
    for h in range(2):
        cols = slice(h * HD, h * HD + HD)
        kw = jnp.concatenate(
            [
                k[128 * n : 128 * n + 128, cols].astype(F32)
                * tt[:, 16 + 8 * h + n : 17 + 8 * h + n]
                for n in range(8)
            ],
            axis=0,
        )
        hi, lo = split(kw)
        st_out[HD * h : HD * h + HD, :] = dot_tn(hi, v[:, cols]) + dot_tn(lo, v[:, cols])
        normers.append(jnp.sum(kw, axis=0, keepdims=True))
    st_out[256:264, :] = jnp.concatenate(
        normers
        + [heads[0][0], heads[1][0], heads[0][1], heads[1][1], last, last],
        axis=0,
    )

    send(st_out, st_twin, sss.at[0], ssr.at[0], sibling)

    arrive(st_twin, sss.at[0], ssr.at[0])
    first_core = c == 0
    mine, twin = st_out[256:264, :], st_twin[256:264, :]
    early = jnp.where(first_core, mine, twin)
    late = jnp.where(first_core, twin, mine)
    goes = early[6:7, :] == late[6:7, :]
    meta = [None] * 8
    for h in range(2):
        span = slice(HD * h, HD * h + HD)
        one = jnp.where(goes, early[2 + h : 3 + h, :] + late[4 + h : 5 + h, :], NEG)
        two = late[2 + h : 3 + h, :]
        stab = jnp.maximum(one, two)
        share_one = jnp.where(goes, jnp.exp(one - stab), 0.0)
        share_two = jnp.exp(two - stab)
        share_mine = jnp.where(first_core, share_one, share_two)
        share_twin = jnp.where(first_core, share_two, share_one)
        mem_out[span, :] = (share_mine * st_out[span, :] + share_twin * st_twin[span, :]).astype(BF)
        meta[h] = share_mine * mine[h : h + 1, :] + share_twin * twin[h : h + 1, :]
        meta[2 + h] = stab
        meta[4 + h] = early[4 + h : 5 + h, :] + late[4 + h : 5 + h, :]
    meta[6] = meta[7] = late[6:7, :]
    meta_out[...] = jnp.concatenate(meta, axis=0)
    head = pl.ds(HD * c, HD)
    for d in range(1, LOOK + 1):
        send(meta_out, meta_in.at[d - 1], sss.at[1], ssr.at[1], chip_ahead(d))
        send(mem_out.at[head], mem_in.at[d - 1, head], sss.at[2], ssr.at[2], chip_ahead(d))

    w_0("sp_1")

    in_q.wait()
    for h in range(2):
        vones[h, :, :HD] = v[:, HD * h : HD * h + HD]
        vones[h, :, HD:] = jnp.ones((T, HD), BF)

    def column(n):
        return jnp.concatenate([tt[:, n : n + 1], tt[:, n + 1 : n + 2]], axis=0)

    for h in range(2):
        cols = slice(h * HD, h * HD + HD)
        for i in range(4):
            at = slice(256 * i, 256 * i + 256)
            m_col, d_col = column(8 * h + 2 * i), column(32 + 2 * i)
            acc = jnp.zeros((256, 2 * HD), F32)
            for j in range(i + 1):
                keys = slice(256 * j, 256 * j + 256)
                a_row, d_row = (
                    jnp.concatenate([ref[n + 2 * j : n + 2 * j + 1, :], ref[n + 2 * j + 1 : n + 2 * j + 2, :]], axis=1)
                    for ref, n in ((arow, 8 * h), (drow, 0))
                )
                ok = d_col == d_row
                if i == j:
                    ok = ok & (
                        lax.broadcasted_iota(jnp.int32, (256, 256), 0)
                        >= lax.broadcasted_iota(jnp.int32, (256, 256), 1)
                    )
                p = jnp.where(ok, dot_nt(q[at, cols], k[keys, cols]) * jnp.exp(a_row - m_col), 0.0)
                hi, lo = split(p)
                acc = acc + (dot(hi, vones[h, keys, :]) + dot(lo, vones[h, keys, :]))
            numden[h, at, :] = acc
    in_og.wait()
    for i in range(4):
        at = slice(256 * i, 256 * i + 256)
        opened[at, :] = 1.0 / (1.0 + jnp.exp(-og[at, :].astype(F32)))

    o_arrive(0, x_l, 0, 64)
    o_send(3, x_l, 0, 64, right)
    o_arrive(1, x_r, 64, 64)
    o_send(3, x_r, 64, 64, left)
    arrive(mem_in.at[:, head], sss.at[2], ssr.at[2])
    for d in range(LOOK):
        send(mem_in.at[d, head], mem_in.at[d, head], sss.at[2], ssr.at[3], sibling)
    arrive(meta_in, sss.at[1], ssr.at[1])
    arrive(mem_in.at[:, pl.ds(HD * (1 - c), HD)], sss.at[2], ssr.at[3])
    second_core = c == 1
    one_back = meta_in[0, 6:7, :]
    carry_doc = jnp.where(second_core, twin[6:7, :], jnp.where(chip > 0, one_back, -1.0))
    scale = HD**-0.5
    memories = []
    for h in range(2):
        passed = jnp.where(second_core, twin[4 + h : 5 + h, :], 0.0)
        levels = [jnp.where(second_core, twin[2 + h : 3 + h, :], NEG)]
        for d in range(1, LOOK + 1):
            ok = (meta_in[d - 1, 6:7, :] == carry_doc) & (chip >= d)
            levels.append(jnp.where(ok, meta_in[d - 1, 2 + h : 3 + h, :] + passed, NEG))
            passed = passed + meta_in[d - 1, 4 + h : 5 + h, :]
        stab = levels[0]
        for level in levels[1:]:
            stab = jnp.maximum(stab, level)
        shares = [jnp.where(level > 0.5 * NEG, jnp.exp(level - stab), 0.0) for level in levels]
        memory = shares[0] * st_twin[HD * h : HD * h + HD, :]
        normer = shares[0] * twin[h : h + 1, :]
        for d in range(1, LOOK + 1):
            memory = memory + shares[d] * mem_in[d - 1, HD * h : HD * h + HD, :].astype(F32)
            normer = normer + shares[d] * meta_in[d - 1, h : h + 1, :]
        memories.append(memory)
        m = heads[h][2]
        goes_on = docs == carry_doc
        both = jnp.where(goes_on, jnp.maximum(m, stab), m)
        vt[8 * h : 8 * h + 8, :] = jnp.exp(m - both) * scale
        vt[16 + 8 * h : 24 + 8 * h, :] = jnp.where(goes_on, jnp.exp(stab - both), 0.0) * scale
        vt[32 + 8 * h : 40 + 8 * h, :] = jnp.broadcast_to(normer, (8, HD))
    tt[...] = vt[...].T
    for h in range(2):
        cols = slice(h * HD, h * HD + HD)
        normer = jnp.broadcast_to(tt[:, 32 + 8 * h : 33 + 8 * h], (HD, HD))
        parts = [jnp.concatenate(pair, axis=1) for pair in zip(split(memories[h]), split(normer))]
        for i in range(4):
            at = slice(256 * i, 256 * i + 256)
            scale_in, scale_by = column(8 * h + 2 * i), column(16 + 8 * h + 2 * i)
            queries = q[at, cols]
            both = scale_in * numden[h, at, :] + scale_by * (dot(queries, parts[0]) + dot(queries, parts[1]))
            cell = both[:, :HD] / jnp.maximum(jnp.abs(both[:, HD:]), 1.0)
            gate_out[i, :, cols] = (cell * opened[at, cols]).astype(BF)

    def half_of(ref, slot, half):
        return ref.at[slot, pl.ds(128 * half, 128)]

    onward, behind = {"tp": lax.rem(x + 1 + 2 * c, 4)}, lax.rem(x + 3 + 2 * c, 4)

    def g_send(n, half, src, dst, device):
        send(half_of(*src, half), half_of(*dst, half), ass, asr.at[2 * n + half], device)

    def g_start(half):
        g_send(0, half, (gate_out, x_a), (gate_relay, 0), onward)
        g_send(1, half, (gate_out, x_r), (gate_in, x), right)
        g_send(1, half, (gate_out, x_l), (gate_in, x), left)

    g_start(0)

    def relay(half):
        arrive(half_of(gate_relay, 0, half), ass, asr.at[half])
        g_send(1, half, (gate_relay, 0), (gate_in, behind), onward)

    gate_in[x] = gate_out[x]

    w_1(0)
    w_pass_on(1, 0)
    w_1(1)
    w_pass_on(0, 0)
    o_arrive(2, x_l, 0, 128)
    for slot in (x_l, x_r):
        o_send(4, slot, 0, 128, sibling)
    w_1(2)
    w_pass_on(3, 0)
    w_1(3)
    w_pass_on(2, 0)
    o_arrive(3, x_a, 0, 128)
    o_send(4, x_a, 0, 128, sibling)
    relay(0)
    g_start(1)
    arrive(ow.at[pl.ds(0, 3), pl.ds((1 - c) * 128, 128)], oss, osr.at[4])
    in_res.wait()

    def r_at(slot, first, count):
        return rows.at[slot, pl.ds(first, count)]

    def r_send(n, slot, first, count, device):
        send(r_at(slot, first, count), r_at(slot, first, count), gss, gsr.at[n], device)

    def r_arrive(n, slot, first, count):
        arrive(r_at(slot, first, count), gss, gsr.at[n])

    def output_rows(half, devices):
        span = pl.ds(128 * half, 128)
        cells = jnp.concatenate([gate_in[n, span] for n in range(4)], axis=1)

        def project(n, squares):
            cols = pl.ds(pl.multiple_of(n * 256, 256), 256)
            acc = res[span, cols].astype(F32) + dot(cells, ow[:, :, cols].reshape(1024, 256))
            stream[span, cols] = acc
            gain_row = jnp.concatenate([gsc[pl.ds(2 * n, 1), :], gsc[pl.ds(2 * n + 1, 1), :]], axis=1)
            rows[x, span, cols] = (acc * gain_row).astype(BF)
            return squares + (acc[:, :128] * acc[:, :128] + acc[:, 128:] * acc[:, 128:])

        squares = jnp.zeros((128, 128), F32)
        for part_of in range(4):
            squares = lax.fori_loop(2 * part_of, 2 * part_of + 2, project, squares)
            cols = pl.ds(512 * part_of, 512)
            for n, first, count, device in devices:
                ref = rows.at[x, pl.ds(128 * half + first, count), cols]
                send(ref, ref, gss, gsr.at[n], device)
        inverse = lax.rsqrt(jnp.sum(squares, axis=1, keepdims=True) / D + NORM_EPS)
        at = pl.ds(8 * half, 8)
        inverses[x, at] = jnp.broadcast_to(inverse, (128, 128)).T[0:8, :]
        for device in (right, left, across):
            send(inverses.at[x, at], inverses.at[x, at], iss, isr, device)

    def gated_rows(half):
        arrive(gate_in.at[pl.ds(0, 3), pl.ds(128 * half, 128)], ass, asr.at[2 + half])

    gated_rows(0)
    relay(1)
    output_rows(0, ((0, 0, 128, right), (1, 0, 128, left)))
    gated_rows(1)
    output_rows(1, ((1, 0, 128, right), (2, 0, 64, left), (3, 64, 64, left)))

    w_2(0)
    w_2(1)
    for n in (1, 2):
        w_pass_on(0, n)
        w_pass_on(1, n)
    w_finish(0, 0)
    w_finish(1, 0)
    w_2(2)
    w_2(3)
    w_pass_on(1, 3)
    w_pass_on(0, 3)
    for n in (1, 2):
        w_pass_on(2, n)
        w_pass_on(3, n)
    r_arrive(0, x_l, 0, 128)
    r_send(4, x_l, 0, 128, right)
    for n in (1, 2):
        w_finish(0, n)
        w_finish(1, n)
    w_pass_on(3, 3)
    w_pass_on(2, 3)
    w_finish(0, 3)
    w_finish(1, 3)
    r_arrive(2, x_r, 128, 64)
    r_send(4, x_r, 128, 64, left)
    for n in range(3):
        w_finish(2, n)
        w_finish(3, n)
    r_arrive(3, x_r, 192, 64)
    r_send(4, x_r, 192, 64, left)
    w_twin(0)

    arrive(inverses.at[pl.ds(0, 3)], iss, isr)
    up_half, low_half = pl.ds(0, 128), pl.ds(128, 128)

    def widen(n, pieces, first=0, last=NJ):
        for m, (slot, half) in enumerate(pieces):
            row_of = inverses[slot, pl.ds(half.start // 16, 8)][0:1, :]
            factor[128 * m : 128 * m + 128, :] = jnp.broadcast_to(row_of, (128, 128)).T

        def one(j, carry):
            both = jnp.concatenate(
                [w[2 * j].reshape(D, 128), w[2 * j + 1].reshape(D, 128)], axis=1
            )
            acts = dot(jnp.concatenate([rows[piece] for piece in pieces], axis=0), both)
            gate_act, up_act = acts[:, :128] * factor[...], acts[:, 128:] * factor[...]
            cols = pl.ds(pl.multiple_of(j * 128, 128), 128)
            hid[n, :, cols] = (gate_act * (1.0 / (1.0 + jnp.exp(-gate_act))) * up_act).astype(BF)
            return carry

        lax.fori_loop(first, last, one, 0)

    def narrow(n, store, first=0, last=D // 256):
        def one(t, carry):
            down = jnp.concatenate(
                [
                    w[2 * NJ + j, t // 2, pl.ds(2 * lax.rem(t, 2), 2)].reshape(256, 128)
                    for j in range(NJ)
                ],
                axis=1,
            )
            store(pl.ds(pl.multiple_of(t * 256, 256), 256), dot_nt(hid[n], down))
            return carry

        lax.fori_loop(first, last, one, 0)

    def keep(n):
        def store(cols, value):
            part[n, :, cols] = value.astype(BF)

        return store

    def p_send(n, src, dst, device):
        send(src, dst, rss, rsr.at[n], device)

    def p_arrive(n, ref):
        arrive(ref, rss, rsr.at[n])

    def piece(ref, slot, half, side):
        return ref.at[slot, half, pl.ds(1024 * side, 1024)]

    pieces = ((x_l, up_half), (x_r, low_half))
    widen(0, pieces, 0, 6)
    w_finish(2, 3)
    w_finish(3, 3)
    widen(0, pieces, 6, NJ)
    w_twin(1)
    for t in range(4):
        narrow(0, keep(0), 2 * t, 2 * t + 2)
        at = pl.ds(512 * t, 512)
        p_send(t // 2, part.at[0, low_half, at], fin.at[0, low_half, at], right)
        p_send(t // 2, part.at[0, up_half, at], fin.at[1, up_half, at], left)
    r_arrive(4, x_a, 0, R)
    widen(2, ((x_a, up_half), (x_a, low_half)))
    for side in range(2):
        narrow(2, keep(2), 4 * side, 4 * side + 4)
        p_send(2 + side, piece(part, 2, up_half, side), piece(mid, 0, up_half, side), right)
        p_send(2 + side, piece(part, 2, low_half, side), piece(mid, 1, up_half, side), left)
    r_arrive(1, x_r, 0, R)
    widen(1, ((x_r, up_half), (x_l, low_half)))
    narrow(1, keep(1))

    def pass_sum(side):
        at = pl.ds(1024 * side, 1024)
        p_arrive(2 + side, mid.at[:, :, at])
        part[1, up_half, at] = (part[1, up_half, at].astype(F32) + mid[0, :, at].astype(F32)).astype(BF)
        p_send(side, piece(part, 1, up_half, side), piece(fin, 0, up_half, side), right)
        part[1, low_half, at] = (part[1, low_half, at].astype(F32) + mid[1, :, at].astype(F32)).astype(BF)
        p_send(side, piece(part, 1, low_half, side), piece(fin, 1, low_half, side), left)

    pass_sum(0)
    widen(3, ((x, up_half), (x, low_half)))
    pass_sum(1)
    def own(cols, value):
        stream[:, cols] = stream[:, cols] + 0.5 * value

    narrow(3, own)
    for side in range(2):
        at = pl.ds(1024 * side, 1024)
        p_arrive(side, fin.at[:, :, at])

        def finish(n, carry):
            cols = pl.ds(pl.multiple_of(n * 256, 256), 256)
            others = fin[0, :, cols].astype(F32) + fin[1, :, cols].astype(F32)
            out[:, cols] = (stream[:, cols] + 0.5 * others).astype(BF)
            return carry

        lax.fori_loop(4 * side, 4 * side + 4, finish, 0)

    drain(w.at[:, pl.ds(0, 1), pl.ds(0, 1)], wss.at[0])
    drain(w.at[:, pl.ds(0, 1), pl.ds(0, 1), pl.ds(0, 1)], wss.at[1])
    drain(w.at[:, pl.ds(0, 1)], wss.at[2])
    drain(w.at[:, pl.ds(0, 1), :, pl.ds(0, 1)], wss.at[3])
    drain(w.at[pl.ds(0, 2 * NJ), :, :, pl.ds(0, 1)], wss.at[4])
    drain(w.at[pl.ds(0, NJ), :, :, pl.ds(0, 1)], wss.at[5])
    drain(ow.at[pl.ds(0, 3)], oss)
    drain(st_out, sss.at[0])
    drain(meta_in, sss.at[1])
    drain(mem_in, sss.at[2])
    drain(gate_in, ass)
    drain(rows.at[pl.ds(0, 3)], gss)
    drain(inverses.at[pl.ds(0, 3)], iss)
    drain(part, rss)


def body(
    query_rows,
    key_rows,
    value_rows,
    input_gate,
    forget_gate,
    output_gate,
    documents,
    residual,
    out_weight,
    norm_gain,
    gate_weight,
    up_weight,
    down_weight,
):
    vmem = pl.BlockSpec(memory_space=pltpu.VMEM)
    hbm = pl.BlockSpec(memory_space=pl.ANY)
    dma = pltpu.SemaphoreType.DMA
    return pl.pallas_call(
        kernel,
        out_shape=pltpu.VMEM((R, D), BF),
        in_specs=[hbm] * 13,
        out_specs=vmem,
        scratch_shapes=[
            pltpu.VMEM((2, T), F32),
            pltpu.VMEM((2, T), F32),
            pltpu.VMEM((8, 128), jnp.int32),
            pltpu.VMEM((16, 128), BF),
            pltpu.VMEM((T, 256), BF),
            pltpu.VMEM((T, 256), BF),
            pltpu.VMEM((T, 256), BF),
            pltpu.VMEM((T, 256), BF),
            pltpu.VMEM((R, D), BF),
            pltpu.VMEM((64, FD), BF),
            pltpu.VMEM((64, FD), BF),
            pltpu.VMEM((64, FD), BF),
            pltpu.VMEM((TILES, 4, 4, 2, 64, 128), BF),
            pltpu.VMEM((4, 256, D), BF),
            pltpu.VMEM((264, 128), F32),
            pltpu.VMEM((264, 128), F32),
            pltpu.VMEM((256, 128), BF),
            pltpu.VMEM((8, 128), F32),
            pltpu.VMEM((LOOK, 256, 128), BF),
            pltpu.VMEM((LOOK, 8, 128), F32),
            pltpu.VMEM((4, R, 256), BF),
            pltpu.VMEM((4, R, 256), BF),
            pltpu.VMEM((1, R, 256), BF),
            pltpu.VMEM((R, D), F32),
            pltpu.VMEM((4, R, D), BF),
            pltpu.VMEM((4, R, FD), BF),
            pltpu.VMEM((3, R, D), BF),
            pltpu.VMEM((2, 128, D), BF),
            pltpu.VMEM((2, R, D), BF),
            pltpu.VMEM((128, 128), F32),
            pltpu.VMEM((128, 128), F32),
            pltpu.VMEM((16, 128), F32),
            pltpu.VMEM((8, 128), F32),
            pltpu.VMEM((16, 128), F32),
            pltpu.VMEM((2, T, 256), BF),
            pltpu.VMEM((2, T, 256), F32),
            pltpu.VMEM((T, 256), F32),
            pltpu.VMEM((4, 16, 128), F32),
            pltpu.VMEM((R, 128), F32),
            dma((13,)),
            dma((6,)),
            dma((4, 17)),
            dma(()),
            dma((5,)),
            dma((3,)),
            dma((4,)),
            dma(()),
            dma((4,)),
            dma(()),
            dma((5,)),
            dma(()),
            dma(()),
            dma(()),
            dma((4,)),
        ],
        compiler_params=pltpu.CompilerParams(
            collective_id=0, has_side_effects=True, vmem_limit_bytes=62 * 1024 * 1024
        ),
    )(
        input_gate,
        forget_gate,
        documents.reshape(8, 128),
        norm_gain.reshape(16, 128),
        query_rows,
        key_rows,
        value_rows,
        output_gate,
        residual,
        out_weight,
        gate_weight,
        up_weight,
        down_weight.T,
    )


def solution(mesh):
    torus = Mesh(mesh.devices.reshape(4, 4, 2, mesh.shape["tp"]), SP_TP)
    in_specs = (
        P(SP, "tp"),
        P(SP, "tp"),
        P(SP, "tp"),
        P("tp", SP),
        P("tp", SP),
        P(SP, "tp"),
        P(SP),
        P(SP_TP, None),
        P("tp", None),
        P(),
        P(SP, "tp"),
        P(SP, "tp"),
        P("tp", SP),
    )
    out_specs = P(SP_TP, None)
    return jax.shard_map(body, mesh=torus, in_specs=in_specs, out_specs=out_specs, check_vma=False)
```

```python
import jax
import jax.numpy as jnp
from jax import lax
from jax.experimental import pallas as pl
from jax.experimental.pallas import tpu as pltpu
from jax.sharding import Mesh
from jax.sharding import PartitionSpec as P

HD = 128
SP = ("sp_0", "sp_1", "sp_2")
SP_TP = ("sp_0", "sp_1", "sp_2", "tp")
MESH = pl.DeviceIdType.MESH
BF = jnp.bfloat16
F32 = jnp.float32

NORM_EPS = 1e-06
NEG = -1e30
T = 1024
R = 256
D = 2048
FD = 1408
NJ = FD // 128
LOOK = 3
TILES = 3 * NJ
PARTS = ((0, 9, 5), (9, 13, 6), (22, 5, 3), (27, 6, 3))


def dot(a, b):
    return jnp.dot(a, b, preferred_element_type=F32)


def dot_nt(a, b):
    return lax.dot_general(a, b, (((1,), (1,)), ((), ())), preferred_element_type=F32)


def dot_tn(a, b):
    return lax.dot_general(a, b, (((0,), (0,)), ((), ())), preferred_element_type=F32)


def split(a):
    hi = a.astype(BF)
    return hi, (a - hi.astype(F32)).astype(BF)


def kernel(
    in_gate_hbm,
    forget_hbm,
    doc_hbm,
    gain_hbm,
    q_hbm,
    k_hbm,
    v_hbm,
    og_hbm,
    res_hbm,
    ow_hbm,
    wg_hbm,
    wu_hbm,
    wd_hbm,
    out,
    in_gate,
    forget,
    doc_ref,
    gain,
    q,
    k,
    v,
    og,
    res,
    wg,
    wu,
    wd,
    w,
    ow,
    st_out,
    st_twin,
    mem_out,
    meta_out,
    mem_in,
    meta_in,
    gate_out,
    gate_in,
    gate_relay,
    stream,
    rows,
    hid,
    part,
    mid,
    fin,
    vt,
    tt,
    arow,
    drow,
    gsc,
    vones,
    numden,
    opened,
    inverses,
    factor,
    lsem,
    wss,
    wsr,
    oss,
    osr,
    sss,
    ssr,
    ass,
    asr,
    gss,
    gsr,
    iss,
    isr,
    rss,
    rsr,
):
    z, y, c, x = (lax.axis_index(n) for n in SP_TP)

    def step(a, by):
        return lax.rem(a + by + 8, 4)

    chip = z * 4 + y

    def chip_ahead(by):
        i = lax.rem(chip + by + 16, 16)
        return {"sp_0": i // 4, "sp_1": lax.rem(i, 4)}

    sibling = {"sp_2": 1 - c}
    peers = [sibling]
    for name, at in (("sp_0", z), ("sp_1", y), ("tp", x)):
        peers += [{name: step(at, 1)}, {name: step(at, -1)}]
    peers += [{"tp": step(x, 2)}]
    for d in range(1, LOOK + 1):
        peers += [chip_ahead(d), chip_ahead(-d)]

    barrier = pltpu.get_barrier_semaphore()
    for peer in peers:
        pl.semaphore_signal(barrier, inc=1, device_id=peer, device_id_type=MESH)

    local = []
    for n, (src, dst) in enumerate(
        (
            (in_gate_hbm, in_gate),
            (forget_hbm, forget),
            (doc_hbm, doc_ref),
            (gain_hbm, gain),
            (ow_hbm, ow.at[x]),
            (wg_hbm, wg),
            (wu_hbm, wu),
            (wd_hbm, wd),
            (k_hbm, k),
            (v_hbm, v),
            (q_hbm, q),
            (og_hbm, og),
            (res_hbm, res),
        )
    ):
        copy = pltpu.make_async_copy(src, dst, lsem.at[n])
        copy.start()
        local.append(copy)
    small, (in_ow, in_wg, in_wu, in_wd, in_k, in_v, in_q, in_og, in_res) = local[:4], local[4:]

    def remote(src, dst, send_sem, recv_sem, device):
        return pltpu.make_async_remote_copy(
            src_ref=src,
            dst_ref=dst,
            send_sem=send_sem,
            recv_sem=recv_sem,
            device_id=device,
            device_id_type=MESH,
        )

    def send(*args):
        remote(*args).start()

    def drain(ref, sem):
        remote(ref, ref, sem, lsem.at[0], sibling).wait_send()

    def arrive(ref, send_sem, recv_sem):
        remote(ref, ref, send_sem, recv_sem, sibling).wait_recv()

    def w_axes(p):
        return (("sp_0", z), ("sp_1", y)) if p % 2 == 0 else (("sp_1", y), ("sp_0", z))

    def w_at(p, first, count, uu, vv):
        zz, yy = (uu, vv) if p % 2 == 0 else (vv, uu)
        return w.at[pl.ds(first, count), zz, yy, c]

    def w_send(p, n, first, count, uu, vv, device):
        ref = w_at(p, first, count, uu, vv)
        place = (0, 1, 2, 2)[n] if n < 4 else 3 * (n // 4) + (0, 1, 2, 2)[n % 4]
        group = 2 * (n // 4 > 0) + (n % 4 > 1)
        send(ref, ref, wss.at[group], wsr.at[p, place], device)

    def w_arrive(p, place, uu, vv):
        first, count, _ = PARTS[p]
        arrive(w_at(p, first, count, uu, vv), wss.at[0], wsr.at[p, place])

    LINE = (0, -1, 1, 2)

    def w_spread(p, n):
        (_, uu), (vn, vv) = w_axes(p)
        first, count, _ = PARTS[p]
        for s, by in ((0, 1), (1, -1)):
            w_send(p, 4 + 4 * n + s, first, count, step(uu, LINE[n]), vv, {vn: step(vv, by)})

    def w_pass_on(p, n):
        (_, uu), (vn, vv) = w_axes(p)
        first, count, half = PARTS[p]
        k_at = step(uu, LINE[n])
        w_arrive(p, 3 + 3 * n, k_at, step(vv, -1))
        w_send(p, 6 + 4 * n, first, half, k_at, step(vv, -1), {vn: step(vv, 1)})
        w_arrive(p, 4 + 3 * n, k_at, step(vv, 1))
        w_send(p, 7 + 4 * n, first + half, count - half, k_at, step(vv, 1), {vn: step(vv, -1)})
        for by in (0, -1, 1) if p < 2 else ():
            w_hand_over(p, n, by)

    def w_hand_over(p, n, by):
        (_, uu), (_, vv) = w_axes(p)
        first, count, _ = PARTS[p]
        ref = w_at(p, first, count, step(uu, LINE[n]), step(vv, by))
        send(ref, ref, wss.at[4 + p // 2], wsr.at[0, 15 + p // 2], sibling)

    def w_twin(kind):
        first, count = ((0, 2 * NJ), (2 * NJ, NJ))[kind]
        arrive(w.at[pl.ds(first, count), :, :, 1 - c], wss.at[0], wsr.at[0, 15 + kind])

    def w_finish(p, n):
        (_, uu), (_, vv) = w_axes(p)
        w_arrive(p, 5 + 3 * n, step(uu, LINE[n]), step(vv, 2))
        for by in (2,) if p < 2 else (0, -1, 1, 2):
            w_hand_over(p, n, by)

    def w_0(name):
        for p in (0, 1, 2, 3) if name == "sp_0" else (1, 0, 3, 2):
            (un, uu), (_, vv) = w_axes(p)
            first, count, _ = PARTS[p]
            if un == name:
                for n, by in ((0, 1), (1, -1)):
                    w_send(p, n, first, count, uu, vv, {un: step(uu, by)})
            else:
                w_spread(p, 0)

    def w_1(p):
        (un, uu), (_, vv) = w_axes(p)
        first, count, half = PARTS[p]
        w_arrive(p, 0, step(uu, -1), vv)
        w_send(p, 2, first, half, step(uu, -1), vv, {un: step(uu, 1)})
        w_spread(p, 1)
        w_arrive(p, 1, step(uu, 1), vv)
        w_send(p, 3, first + half, count - half, step(uu, 1), vv, {un: step(uu, -1)})
        w_spread(p, 2)

    def w_2(p):
        (_, uu), (_, vv) = w_axes(p)
        w_arrive(p, 2, step(uu, 2), vv)
        w_spread(p, 3)

    right, left, across = {"tp": step(x, 1)}, {"tp": step(x, -1)}, {"tp": step(x, 2)}
    x_r, x_l, x_a = step(x, 1), step(x, -1), step(x, 2)

    def o_at(slot, part_first, count):
        return ow.at[slot, pl.ds(c * 128 + part_first, count)]

    def o_send(n, slot, first, count, device):
        send(o_at(slot, first, count), o_at(slot, first, count), oss, osr.at[n], device)


    def o_arrive(n, slot, first, count):
        arrive(o_at(slot, first, count), oss, osr.at[n])

    pl.semaphore_wait(barrier, len(peers))
    in_ow.wait()
    o_send(0, x, 0, 64, right)
    o_send(1, x, 64, 64, left)
    o_send(2, x, 64, 64, right)
    o_send(2, x, 0, 64, left)

    in_wg.wait()
    in_wu.wait()
    in_wd.wait()
    for j in range(NJ):
        cols = slice(128 * j, 128 * j + 128)
        w[2 * j, z, y, c] = wg[:, cols]
        w[2 * j + 1, z, y, c] = wu[:, cols]
        w[2 * NJ + j, z, y, c] = wd[:, cols]

    w_0("sp_0")

    for copy in small:
        copy.wait()
    lane = lax.broadcasted_iota(jnp.int32, (8, 128), 1)
    row = lax.broadcasted_iota(jnp.int32, (8, 128), 0)
    docs = doc_ref[...].astype(F32)
    drow[...] = docs
    gsc[...] = gain[...].astype(F32)
    last_lane = jnp.broadcast_to(docs[:, 127:128], (8, 128))
    heads = []
    vt[...] = jnp.zeros_like(vt)

    def eight_rows(ref, h):
        return jnp.concatenate([ref[h : h + 1, 128 * n : 128 * n + 128] for n in range(8)], axis=0)

    for h in range(2):
        cum = eight_rows(forget, h)
        cum = jnp.minimum(cum, 0.0) - jnp.log1p(jnp.exp(-jnp.abs(cum)))
        for s in (1, 2, 4, 8, 16, 32, 64):
            cum = cum + jnp.where(lane >= s, pltpu.roll(cum, s, 1), 0.0)
        upto = jnp.broadcast_to(cum[:, 127:128], (8, 128))
        for s in (1, 2, 4):
            upto = upto + jnp.where(row >= s, pltpu.roll(upto, s, 0), 0.0)
        cum = cum + jnp.where(row >= 1, pltpu.roll(upto, 1, 0), 0.0)
        a = eight_rows(in_gate, h) - cum
        m = a
        for s in (1, 2, 4, 8, 16, 32, 64):
            ok = (lane >= s) & (pltpu.roll(docs, s, 1) == docs)
            m = jnp.where(ok, jnp.maximum(m, pltpu.roll(m, s, 1)), m)
        e = jnp.broadcast_to(m[:, 127:128], (8, 128))
        for s in (1, 2, 4):
            ok = (row >= s) & (pltpu.roll(last_lane, s, 0) == last_lane)
            e = jnp.where(ok, jnp.maximum(e, pltpu.roll(e, s, 0)), e)
        ok = (row >= 1) & (pltpu.roll(last_lane, 1, 0) == docs)
        m = jnp.where(ok, jnp.maximum(m, pltpu.roll(e, 1, 0)), m)
        top = e[7:8, :]
        last = last_lane[7:8, :]
        weight = jnp.where(docs == last, jnp.exp(a - top), 0.0)
        arow[8 * h : 8 * h + 8, :] = a
        vt[8 * h : 8 * h + 8, :] = m
        vt[16 + 8 * h : 24 + 8 * h, :] = weight
        total = upto[7:8, :]
        heads.append((top + total, total, m))
    vt[32:40, :] = docs
    tt[...] = vt[...].T

    in_k.wait()
    in_v.wait()
    normers = []
    for h in range(2):
        cols = slice(h * HD, h * HD + HD)
        kw = jnp.concatenate(
            [
                k[128 * n : 128 * n + 128, cols].astype(F32)
                * tt[:, 16 + 8 * h + n : 17 + 8 * h + n]
                for n in range(8)
            ],
            axis=0,
        )
        hi, lo = split(kw)
        st_out[HD * h : HD * h + HD, :] = dot_tn(hi, v[:, cols]) + dot_tn(lo, v[:, cols])
        normers.append(jnp.sum(kw, axis=0, keepdims=True))
    st_out[256:264, :] = jnp.concatenate(
        normers
        + [heads[0][0], heads[1][0], heads[0][1], heads[1][1], last, last],
        axis=0,
    )

    send(st_out, st_twin, sss.at[0], ssr.at[0], sibling)

    arrive(st_twin, sss.at[0], ssr.at[0])
    first_core = c == 0
    mine, twin = st_out[256:264, :], st_twin[256:264, :]
    early = jnp.where(first_core, mine, twin)
    late = jnp.where(first_core, twin, mine)
    goes = early[6:7, :] == late[6:7, :]
    meta = [None] * 8
    for h in range(2):
        span = slice(HD * h, HD * h + HD)
        one = jnp.where(goes, early[2 + h : 3 + h, :] + late[4 + h : 5 + h, :], NEG)
        two = late[2 + h : 3 + h, :]
        stab = jnp.maximum(one, two)
        share_one = jnp.where(goes, jnp.exp(one - stab), 0.0)
        share_two = jnp.exp(two - stab)
        share_mine = jnp.where(first_core, share_one, share_two)
        share_twin = jnp.where(first_core, share_two, share_one)
        mem_out[span, :] = (share_mine * st_out[span, :] + share_twin * st_twin[span, :]).astype(BF)
        meta[h] = share_mine * mine[h : h + 1, :] + share_twin * twin[h : h + 1, :]
        meta[2 + h] = stab
        meta[4 + h] = early[4 + h : 5 + h, :] + late[4 + h : 5 + h, :]
    meta[6] = meta[7] = late[6:7, :]
    meta_out[...] = jnp.concatenate(meta, axis=0)
    head = pl.ds(HD * c, HD)
    for d in range(1, LOOK + 1):
        send(meta_out, meta_in.at[d - 1], sss.at[1], ssr.at[1], chip_ahead(d))
        send(mem_out.at[head], mem_in.at[d - 1, head], sss.at[2], ssr.at[2], chip_ahead(d))

    w_0("sp_1")

    in_q.wait()
    for h in range(2):
        vones[h, :, :HD] = v[:, HD * h : HD * h + HD]
        vones[h, :, HD:] = jnp.ones((T, HD), BF)

    def column(n):
        return jnp.concatenate([tt[:, n : n + 1], tt[:, n + 1 : n + 2]], axis=0)

    for h in range(2):
        cols = slice(h * HD, h * HD + HD)
        for i in range(4):
            at = slice(256 * i, 256 * i + 256)
            m_col, d_col = column(8 * h + 2 * i), column(32 + 2 * i)
            acc = jnp.zeros((256, 2 * HD), F32)
            for j in range(i + 1):
                keys = slice(256 * j, 256 * j + 256)
                a_row, d_row = (
                    jnp.concatenate([ref[n + 2 * j : n + 2 * j + 1, :], ref[n + 2 * j + 1 : n + 2 * j + 2, :]], axis=1)
                    for ref, n in ((arow, 8 * h), (drow, 0))
                )
                ok = d_col == d_row
                if i == j:
                    ok = ok & (
                        lax.broadcasted_iota(jnp.int32, (256, 256), 0)
                        >= lax.broadcasted_iota(jnp.int32, (256, 256), 1)
                    )
                p = jnp.where(ok, dot_nt(q[at, cols], k[keys, cols]) * jnp.exp(a_row - m_col), 0.0)
                hi, lo = split(p)
                acc = acc + (dot(hi, vones[h, keys, :]) + dot(lo, vones[h, keys, :]))
            numden[h, at, :] = acc
    in_og.wait()
    for i in range(4):
        at = slice(256 * i, 256 * i + 256)
        opened[at, :] = 1.0 / (1.0 + jnp.exp(-og[at, :].astype(F32)))

    o_arrive(0, x_l, 0, 64)
    o_send(3, x_l, 0, 64, right)
    o_arrive(1, x_r, 64, 64)
    o_send(5, x_r, 64, 64, left)
    arrive(mem_in.at[:, head], sss.at[2], ssr.at[2])
    for d in range(LOOK):
        send(mem_in.at[d, head], mem_in.at[d, head], sss.at[2], ssr.at[3], sibling)
    arrive(meta_in, sss.at[1], ssr.at[1])
    arrive(mem_in.at[:, pl.ds(HD * (1 - c), HD)], sss.at[2], ssr.at[3])
    second_core = c == 1
    one_back = meta_in[0, 6:7, :]
    carry_doc = jnp.where(second_core, twin[6:7, :], jnp.where(chip > 0, one_back, -1.0))
    scale = HD**-0.5
    memories = []
    for h in range(2):
        passed = jnp.where(second_core, twin[4 + h : 5 + h, :], 0.0)
        levels = [jnp.where(second_core, twin[2 + h : 3 + h, :], NEG)]
        for d in range(1, LOOK + 1):
            ok = (meta_in[d - 1, 6:7, :] == carry_doc) & (chip >= d)
            levels.append(jnp.where(ok, meta_in[d - 1, 2 + h : 3 + h, :] + passed, NEG))
            passed = passed + meta_in[d - 1, 4 + h : 5 + h, :]
        stab = levels[0]
        for level in levels[1:]:
            stab = jnp.maximum(stab, level)
        shares = [jnp.where(level > 0.5 * NEG, jnp.exp(level - stab), 0.0) for level in levels]
        memory = shares[0] * st_twin[HD * h : HD * h + HD, :]
        normer = shares[0] * twin[h : h + 1, :]
        for d in range(1, LOOK + 1):
            memory = memory + shares[d] * mem_in[d - 1, HD * h : HD * h + HD, :].astype(F32)
            normer = normer + shares[d] * meta_in[d - 1, h : h + 1, :]
        memories.append(memory)
        m = heads[h][2]
        goes_on = docs == carry_doc
        both = jnp.where(goes_on, jnp.maximum(m, stab), m)
        vt[8 * h : 8 * h + 8, :] = jnp.exp(m - both) * scale
        vt[16 + 8 * h : 24 + 8 * h, :] = jnp.where(goes_on, jnp.exp(stab - both), 0.0) * scale
        vt[32 + 8 * h : 40 + 8 * h, :] = jnp.broadcast_to(normer, (8, HD))
    tt[...] = vt[...].T
    for h in range(2):
        cols = slice(h * HD, h * HD + HD)
        normer = jnp.broadcast_to(tt[:, 32 + 8 * h : 33 + 8 * h], (HD, HD))
        parts = [jnp.concatenate(pair, axis=1) for pair in zip(split(memories[h]), split(normer))]
        for i in range(4):
            at = slice(256 * i, 256 * i + 256)
            scale_in, scale_by = column(8 * h + 2 * i), column(16 + 8 * h + 2 * i)
            queries = q[at, cols]
            both = scale_in * numden[h, at, :] + scale_by * (dot(queries, parts[0]) + dot(queries, parts[1]))
            cell = both[:, :HD] / jnp.maximum(jnp.abs(both[:, HD:]), 1.0)
            gate_out[i, :, cols] = (cell * opened[at, cols]).astype(BF)

    def half_of(ref, slot, half):
        return ref.at[slot, pl.ds(128 * half, 128)]

    onward, behind = {"tp": lax.rem(x + 1 + 2 * c, 4)}, lax.rem(x + 3 + 2 * c, 4)

    def g_send(n, half, src, dst, device):
        send(half_of(*src, half), half_of(*dst, half), ass, asr.at[2 * n + half], device)

    def g_start(half):
        g_send(0, half, (gate_out, x_a), (gate_relay, 0), onward)
        g_send(1, half, (gate_out, x_r), (gate_in, x), right)
        g_send(1, half, (gate_out, x_l), (gate_in, x), left)

    g_start(0)

    def relay(half):
        arrive(half_of(gate_relay, 0, half), ass, asr.at[half])
        g_send(1, half, (gate_relay, 0), (gate_in, behind), onward)

    gate_in[x] = gate_out[x]

    w_1(0)
    w_pass_on(1, 0)
    w_1(1)
    w_pass_on(0, 0)
    o_arrive(2, x_l, 0, 128)
    for slot in (x_l, x_r):
        o_send(4, slot, 0, 128, sibling)
    w_1(2)
    w_pass_on(3, 0)
    w_1(3)
    w_pass_on(2, 0)
    o_arrive(3, x_a, 0, 64)
    o_send(4, x_a, 0, 64, sibling)
    o_arrive(5, x_a, 64, 64)
    o_send(4, x_a, 64, 64, sibling)
    relay(0)
    g_start(1)
    arrive(ow.at[pl.ds(0, 3), pl.ds((1 - c) * 128, 128)], oss, osr.at[4])
    in_res.wait()

    def r_at(slot, first, count):
        return rows.at[slot, pl.ds(first, count)]

    def r_send(n, slot, first, count, device):
        send(r_at(slot, first, count), r_at(slot, first, count), gss, gsr.at[n], device)

    def r_arrive(n, slot, first, count):
        arrive(r_at(slot, first, count), gss, gsr.at[n])

    def output_rows(half, devices):
        span = pl.ds(128 * half, 128)
        cells = jnp.concatenate([gate_in[n, span] for n in range(4)], axis=1)

        def project(n, squares):
            cols = pl.ds(pl.multiple_of(n * 256, 256), 256)
            acc = res[span, cols].astype(F32) + dot(cells, ow[:, :, cols].reshape(1024, 256))
            stream[span, cols] = acc
            gain_row = jnp.concatenate([gsc[pl.ds(2 * n, 1), :], gsc[pl.ds(2 * n + 1, 1), :]], axis=1)
            rows[x, span, cols] = (acc * gain_row).astype(BF)
            return squares + (acc[:, :128] * acc[:, :128] + acc[:, 128:] * acc[:, 128:])

        squares = jnp.zeros((128, 128), F32)
        for part_of in range(4):
            squares = lax.fori_loop(2 * part_of, 2 * part_of + 2, project, squares)
            cols = pl.ds(512 * part_of, 512)
            for n, first, count, device in devices:
                ref = rows.at[x, pl.ds(128 * half + first, count), cols]
                send(ref, ref, gss, gsr.at[n], device)
        inverse = lax.rsqrt(jnp.sum(squares, axis=1, keepdims=True) / D + NORM_EPS)
        at = pl.ds(8 * half, 8)
        inverses[x, at] = jnp.broadcast_to(inverse, (128, 128)).T[0:8, :]
        for device in (right, left, across):
            send(inverses.at[x, at], inverses.at[x, at], iss, isr, device)

    def gated_rows(half):
        arrive(gate_in.at[pl.ds(0, 3), pl.ds(128 * half, 128)], ass, asr.at[2 + half])

    gated_rows(0)
    relay(1)
    output_rows(0, ((0, 0, 128, right), (1, 0, 128, left)))
    gated_rows(1)
    output_rows(1, ((1, 0, 128, right), (2, 0, 64, left), (3, 64, 64, left)))

    w_2(0)
    w_2(1)
    for n in (1, 2):
        w_pass_on(0, n)
        w_pass_on(1, n)
    w_finish(0, 0)
    w_finish(1, 0)
    w_2(2)
    w_2(3)
    w_pass_on(1, 3)
    w_pass_on(0, 3)
    for n in (1, 2):
        w_pass_on(2, n)
        w_pass_on(3, n)
    r_arrive(0, x_l, 0, 128)
    r_send(4, x_l, 0, 128, right)
    for n in (1, 2):
        w_finish(0, n)
        w_finish(1, n)
    w_pass_on(3, 3)
    w_pass_on(2, 3)
    w_finish(0, 3)
    w_finish(1, 3)
    r_arrive(2, x_r, 128, 64)
    r_send(4, x_r, 128, 64, left)
    for n in range(3):
        w_finish(2, n)
        w_finish(3, n)
    r_arrive(3, x_r, 192, 64)
    r_send(4, x_r, 192, 64, left)
    w_twin(0)

    arrive(inverses.at[pl.ds(0, 3)], iss, isr)
    up_half, low_half = pl.ds(0, 128), pl.ds(128, 128)

    def widen(n, pieces, first=0, last=NJ):
        for m, (slot, half) in enumerate(pieces):
            row_of = inverses[slot, pl.ds(half.start // 16, 8)][0:1, :]
            factor[128 * m : 128 * m + 128, :] = jnp.broadcast_to(row_of, (128, 128)).T

        def one(j, carry):
            both = jnp.concatenate(
                [w[2 * j].reshape(D, 128), w[2 * j + 1].reshape(D, 128)], axis=1
            )
            acts = dot(jnp.concatenate([rows[piece] for piece in pieces], axis=0), both)
            gate_act, up_act = acts[:, :128] * factor[...], acts[:, 128:] * factor[...]
            cols = pl.ds(pl.multiple_of(j * 128, 128), 128)
            hid[n, :, cols] = (gate_act * (1.0 / (1.0 + jnp.exp(-gate_act))) * up_act).astype(BF)
            return carry

        lax.fori_loop(first, last, one, 0)

    def narrow(n, store, first=0, last=D // 256):
        def one(t, carry):
            down = jnp.concatenate(
                [
                    w[2 * NJ + j, t // 2, pl.ds(2 * lax.rem(t, 2), 2)].reshape(256, 128)
                    for j in range(NJ)
                ],
                axis=1,
            )
            store(pl.ds(pl.multiple_of(t * 256, 256), 256), dot_nt(hid[n], down))
            return carry

        lax.fori_loop(first, last, one, 0)

    def keep(n):
        def store(cols, value):
            part[n, :, cols] = value.astype(BF)

        return store

    def p_send(n, src, dst, device):
        send(src, dst, rss, rsr.at[n], device)

    def p_arrive(n, ref):
        arrive(ref, rss, rsr.at[n])

    def piece(ref, slot, half, side):
        return ref.at[slot, half, pl.ds(1024 * side, 1024)]

    pieces = ((x_l, up_half), (x_r, low_half))
    widen(0, pieces, 0, 6)
    w_finish(2, 3)
    w_finish(3, 3)
    widen(0, pieces, 6, NJ)
    w_twin(1)
    for t in range(4):
        narrow(0, keep(0), 2 * t, 2 * t + 2)
        at = pl.ds(512 * t, 512)
        p_send(t // 2, part.at[0, low_half, at], fin.at[0, low_half, at], right)
        p_send(t // 2, part.at[0, up_half, at], fin.at[1, up_half, at], left)
    r_arrive(4, x_a, 0, R)
    widen(2, ((x_a, up_half), (x_a, low_half)))
    for side in range(2):
        narrow(2, keep(2), 4 * side, 4 * side + 4)
        p_send(2 + side, piece(part, 2, up_half, side), piece(mid, 0, up_half, side), right)
        p_send(2 + side, piece(part, 2, low_half, side), piece(mid, 1, up_half, side), left)
    r_arrive(1, x_r, 0, R)
    widen(1, ((x_r, up_half), (x_l, low_half)))
    narrow(1, keep(1))

    def pass_sum(side):
        at = pl.ds(1024 * side, 1024)
        p_arrive(2 + side, mid.at[:, :, at])
        part[1, up_half, at] = (part[1, up_half, at].astype(F32) + mid[0, :, at].astype(F32)).astype(BF)
        p_send(side, piece(part, 1, up_half, side), piece(fin, 0, up_half, side), right)
        part[1, low_half, at] = (part[1, low_half, at].astype(F32) + mid[1, :, at].astype(F32)).astype(BF)
        p_send(side, piece(part, 1, low_half, side), piece(fin, 1, low_half, side), left)

    pass_sum(0)
    widen(3, ((x, up_half), (x, low_half)))
    pass_sum(1)
    def own(cols, value):
        stream[:, cols] = stream[:, cols] + 0.5 * value

    narrow(3, own)
    for side in range(2):
        at = pl.ds(1024 * side, 1024)
        p_arrive(side, fin.at[:, :, at])

        def finish(n, carry):
            cols = pl.ds(pl.multiple_of(n * 256, 256), 256)
            others = fin[0, :, cols].astype(F32) + fin[1, :, cols].astype(F32)
            out[:, cols] = (stream[:, cols] + 0.5 * others).astype(BF)
            return carry

        lax.fori_loop(4 * side, 4 * side + 4, finish, 0)

    drain(w.at[:, pl.ds(0, 1), pl.ds(0, 1)], wss.at[0])
    drain(w.at[:, pl.ds(0, 1), pl.ds(0, 1), pl.ds(0, 1)], wss.at[1])
    drain(w.at[:, pl.ds(0, 1)], wss.at[2])
    drain(w.at[:, pl.ds(0, 1), :, pl.ds(0, 1)], wss.at[3])
    drain(w.at[pl.ds(0, 2 * NJ), :, :, pl.ds(0, 1)], wss.at[4])
    drain(w.at[pl.ds(0, NJ), :, :, pl.ds(0, 1)], wss.at[5])
    drain(ow.at[pl.ds(0, 3)], oss)
    drain(st_out, sss.at[0])
    drain(meta_in, sss.at[1])
    drain(mem_in, sss.at[2])
    drain(gate_in, ass)
    drain(rows.at[pl.ds(0, 3)], gss)
    drain(inverses.at[pl.ds(0, 3)], iss)
    drain(part, rss)


def body(
    query_rows,
    key_rows,
    value_rows,
    input_gate,
    forget_gate,
    output_gate,
    documents,
    residual,
    out_weight,
    norm_gain,
    gate_weight,
    up_weight,
    down_weight,
):
    vmem = pl.BlockSpec(memory_space=pltpu.VMEM)
    hbm = pl.BlockSpec(memory_space=pl.ANY)
    dma = pltpu.SemaphoreType.DMA
    return pl.pallas_call(
        kernel,
        out_shape=pltpu.VMEM((R, D), BF),
        in_specs=[hbm] * 13,
        out_specs=vmem,
        scratch_shapes=[
            pltpu.VMEM((2, T), F32),
            pltpu.VMEM((2, T), F32),
            pltpu.VMEM((8, 128), jnp.int32),
            pltpu.VMEM((16, 128), BF),
            pltpu.VMEM((T, 256), BF),
            pltpu.VMEM((T, 256), BF),
            pltpu.VMEM((T, 256), BF),
            pltpu.VMEM((T, 256), BF),
            pltpu.VMEM((R, D), BF),
            pltpu.VMEM((64, FD), BF),
            pltpu.VMEM((64, FD), BF),
            pltpu.VMEM((64, FD), BF),
            pltpu.VMEM((TILES, 4, 4, 2, 64, 128), BF),
            pltpu.VMEM((4, 256, D), BF),
            pltpu.VMEM((264, 128), F32),
            pltpu.VMEM((264, 128), F32),
            pltpu.VMEM((256, 128), BF),
            pltpu.VMEM((8, 128), F32),
            pltpu.VMEM((LOOK, 256, 128), BF),
            pltpu.VMEM((LOOK, 8, 128), F32),
            pltpu.VMEM((4, R, 256), BF),
            pltpu.VMEM((4, R, 256), BF),
            pltpu.VMEM((1, R, 256), BF),
            pltpu.VMEM((R, D), F32),
            pltpu.VMEM((4, R, D), BF),
            pltpu.VMEM((4, R, FD), BF),
            pltpu.VMEM((3, R, D), BF),
            pltpu.VMEM((2, 128, D), BF),
            pltpu.VMEM((2, R, D), BF),
            pltpu.VMEM((128, 128), F32),
            pltpu.VMEM((128, 128), F32),
            pltpu.VMEM((16, 128), F32),
            pltpu.VMEM((8, 128), F32),
            pltpu.VMEM((16, 128), F32),
            pltpu.VMEM((2, T, 256), BF),
            pltpu.VMEM((2, T, 256), F32),
            pltpu.VMEM((T, 256), F32),
            pltpu.VMEM((4, 16, 128), F32),
            pltpu.VMEM((R, 128), F32),
            dma((13,)),
            dma((6,)),
            dma((4, 17)),
            dma(()),
            dma((6,)),
            dma((3,)),
            dma((4,)),
            dma(()),
            dma((4,)),
            dma(()),
            dma((5,)),
            dma(()),
            dma(()),
            dma(()),
            dma((4,)),
        ],
        compiler_params=pltpu.CompilerParams(
            collective_id=0, has_side_effects=True, vmem_limit_bytes=62 * 1024 * 1024
        ),
    )(
        input_gate,
        forget_gate,
        documents.reshape(8, 128),
        norm_gain.reshape(16, 128),
        query_rows,
        key_rows,
        value_rows,
        output_gate,
        residual,
        out_weight,
        gate_weight,
        up_weight,
        down_weight.T,
    )


def solution(mesh):
    torus = Mesh(mesh.devices.reshape(4, 4, 2, mesh.shape["tp"]), SP_TP)
    in_specs = (
        P(SP, "tp"),
        P(SP, "tp"),
        P(SP, "tp"),
        P("tp", SP),
        P("tp", SP),
        P(SP, "tp"),
        P(SP),
        P(SP_TP, None),
        P("tp", None),
        P(),
        P(SP, "tp"),
        P(SP, "tp"),
        P("tp", SP),
    )
    out_specs = P(SP_TP, None)
    return jax.shard_map(body, mesh=torus, in_specs=in_specs, out_specs=out_specs, check_vma=False)
```
